128 devices in a mesh: sp: 16 (over z, y), dp: 8 (over x, core).
Axes of the slice: x: 4, y: 4, z: 4, core: 2. Of those that a mesh axis runs over, the one named last changes fastest.
Arguments:
- queries: bfloat16 [8, 2048, 1024], P('dp', 'sp'), may hold values from -6 to 6
- keys: bfloat16 [8, 2048, 256], P('dp', 'sp'), may hold values from -6 to 6
- values: bfloat16 [8, 2048, 256], P('dp', 'sp'), may hold values from -6 to 6
- q_gain: float32 [64], replicated, may hold values from 0.55 to 8
- k_gain: float32 [64], replicated, may hold values from 0.55 to 8
- residual: bfloat16 [8, 2048, 2048], P('dp', 'sp'), may hold values from -6 to 6
- out_weight: bfloat16 [1024, 2048], replicated, may hold values from -0.1875 to 0.1875
- mix_gain: float32 [2048], replicated, may hold values from 0.1 to 1.9
- ffn_gain: float32 [2048], replicated, may hold values from 0.1 to 1.9
- post_gain: float32 [2048], replicated, may hold values from 0.1 to 1.9
- expert_ids: int32 [8, 2048, 2], P('dp', 'sp'), may hold values from 0 to 127, all different within a row; in each aligned block of 128 rows (0 to 127, 128 to 255, ..., all dimensions but the last counted through in order) at most 4 rows name the same one
- expert_gate: float32 [8, 2048, 2], P('dp', 'sp'), may hold values from 0.05 to 1
- w_gate: bfloat16 [128, 2048, 512], P(('sp', 'dp')), may hold values from -0.125 to 0.125
- w_up: bfloat16 [128, 2048, 512], P(('sp', 'dp')), may hold values from -0.125 to 0.125
- w_down: bfloat16 [128, 512, 2048], P(('sp', 'dp')), may hold values from -0.25 to 0.25
Outputs:
- result: bfloat16 [8, 2048, 2048], P('dp', 'sp')
The draws below stay inside these ranges and needn't reach their ends.
Inputs may be any that keep to these rules, and one draw needn't show every extreme that they name: `expert_ids`: each token names 2 different experts; among the 128 tokens of one device no expert is named more than 4 times, and that bound is reached.
All inputs are finite; a program needn't handle non-finite values.
Results may differ from the reference program's by a relative error of at most 0.0085.
The reference program's roundings to bfloat16 on the way count: a program that leaves them out, or rounds other values in their place, can miss the bound.
Values may be sent and summed in bfloat16 or wider, within the bound.
A program may use at most 64 MiB of HBM per device.

```python
import math
import jax
import jax.numpy as jnp
import numpy as np
from jax import lax

D = 2048
HEAD = 64
H_Q = 16
H_KV = 4
DE = 512
TOP = 2
GRID = 64
TOK_DEV = 128
SEQS = 8
LEN = 2048
EXPERTS = 128
CAP = 4
N_SP = 16
N_DP = 8


def key_field(key):
    base = jax.random.normal(jax.random.fold_in(key, 23), (SEQS, LEN, H_KV * HEAD), jnp.float32)
    return jnp.clip(base, -6.0, 6.0)


def draw_keys(key, part):
    return key_field(key).astype(jnp.bfloat16)


def draw_queries(key, part):
    base = jax.random.normal(jax.random.fold_in(key, 11), (SEQS, LEN, H_Q * HEAD), jnp.float32)
    base = jnp.clip(base, -6.0, 6.0)
    return base.astype(jnp.bfloat16)


def draw_q_gain(key, part):
    inner = jax.random.fold_in(key, 41)
    return 1.0 + 0.18 * jnp.clip(jax.random.normal(inner, (HEAD,), jnp.float32), -2.5, 2.5)


def draw_k_gain(key, part):
    inner = jax.random.fold_in(key, 43)
    return 1.0 + 0.18 * jnp.clip(jax.random.normal(inner, (HEAD,), jnp.float32), -2.5, 2.5)


def level_of(own_key, dims, pieces, least, largest):
    level = 1.0
    for dim, blocks in pieces:
        draws = jax.random.uniform(jax.random.fold_in(jax.random.fold_in(own_key, 6), dim), (blocks,), jnp.float32, least / len(pieces), largest / len(pieces))
        level = level * jnp.repeat(jnp.exp(draws), dims[dim] // blocks).reshape((-1,) + (1,) * (len(dims) - 1 - dim))
    return level


def routed_block(own_key, own, number, rows, count, top, reach, lean):
    ranking = jax.random.permutation(own_key, count)
    crowded, ordinary = load_shares(count, rows * top, reach, lean, True), load_shares(count, rows * top, reach, lean, False)
    places = jnp.arange(count)

    def named(lengths, turn):
        used = int((lengths > 0).sum())
        fixed = max(1, used // 4)
        passed = fixed + (places - fixed + turn * (used - fixed)) % max(1, count - fixed)
        return jnp.zeros((count,), jnp.int32).at[ranking[jnp.where(places < fixed, places, passed)]].set(jnp.asarray(lengths, jnp.int32))

    lengths = jnp.where(number % 4 == 0, named(crowded, number // 4), named(ordinary, number - number // 4 - 1))
    mixed = jax.random.permutation(jax.random.fold_in(own, 3), count)
    giver, sink = mixed[0:count // 2 * 2:2], mixed[1:count // 2 * 2:2]
    slack = jnp.minimum(lengths[giver] - 1, reach - lengths[sink]) // 2
    slack = jnp.where((giver == ranking[0]) | (sink == ranking[0]) | (lengths[sink] == 0), 0, jnp.maximum(slack, 0))
    passed = jax.random.randint(jax.random.fold_in(own, 4), (count // 2,), 0, 1 << 20) % (slack + 1)
    lengths = lengths.at[giver].add(-passed).at[sink].add(passed)
    members = jnp.searchsorted(jnp.cumsum(lengths), jnp.arange(rows * top), side="right").astype(jnp.int32)
    listing = members.reshape(top, rows).T
    listing = listing[jax.random.permutation(jax.random.fold_in(own, 1), rows)]
    turn = jax.random.randint(jax.random.fold_in(own, 2), (rows, 1), 0, top)
    return jnp.take_along_axis(listing, (jnp.arange(top)[None, :] + turn) % top, axis=1)


def load_shares(number_of, total, most, slope, full):
    portions = [(1 << 20) // math.isqrt(grade ** slope) + 1 for grade in range(1, number_of + 1)]
    largest = most if full else min(most, max(-(-total // number_of), total * portions[0] // sum(portions)))
    least = 1 if total - largest >= number_of - 1 else 0
    holding, spare = [largest] + [least] * (number_of - 1), total - largest - least * (number_of - 1)
    while spare > 0:
        movable = [i for i in range(1, number_of) if holding[i] < largest] or [i for i in range(1, number_of) if holding[i] < most]
        mass, left = sum([portions[i] for i in movable]), spare
        for i in movable:
            addition = min(most - holding[i], max(1, left * portions[i] // mass), spare)
            holding[i] = holding[i] + addition
            spare = spare - addition
    return np.array(holding)


def scatter_about(stream_key, dims, width, bound, cuts=(), kind=jnp.bfloat16):
    drawn = width * jax.random.normal(stream_key, dims, jnp.float32)
    if cuts:
        drawn = drawn * level_of(stream_key, dims, cuts, -0.22, 0.18)
    return jnp.clip(drawn, -bound, bound).astype(kind)


def setup_inputs(seed: int = 0) -> dict:
    splits = jax.random.split(jax.random.key(seed), 16)
    queries = draw_queries(jax.random.fold_in(splits[15], 71), 0)
    keys = draw_keys(jax.random.fold_in(splits[15], 71), 0)
    values = scatter_about(splits[2], (SEQS, LEN, H_KV * HEAD), 1.0, 6.0, ((0, 8), (1, 16)))
    q_gain = draw_q_gain(jax.random.fold_in(splits[15], 71), 0)
    k_gain = draw_k_gain(jax.random.fold_in(splits[15], 71), 0)
    residual = scatter_about(splits[5], (SEQS, LEN, D), 1.0, 6.0, ((0, 8), (1, 16)))
    out_weight = scatter_about(splits[6], (H_Q * HEAD, D), (H_Q * HEAD) ** -0.5, 0.1875)
    mix_gain = jnp.clip(1.0 + 0.18 * jax.random.normal(splits[7], (D,), jnp.float32), 0.1, 1.9)
    ffn_gain = jnp.clip(1.0 + 0.18 * jax.random.normal(splits[8], (D,), jnp.float32), 0.1, 1.9)
    post_gain = jnp.clip(1.0 + 0.18 * jax.random.normal(splits[9], (D,), jnp.float32), 0.1, 1.9)
    expert_ids_keys = jax.random.split(jax.random.fold_in(splits[10], 1), SEQS * LEN // TOK_DEV)
    expert_ids_turns = jax.random.permutation(jax.random.fold_in(splits[10], 3), SEQS * LEN // TOK_DEV)
    expert_ids = jax.vmap(lambda own, number: routed_block(jax.random.fold_in(splits[10], 2), own, number, TOK_DEV, EXPERTS, TOP, CAP, 2))(expert_ids_keys, expert_ids_turns).reshape((SEQS, LEN, TOP))
    expert_gate = jnp.clip(jnp.exp(math.log(1.0) - 2.9957323 * jax.random.uniform(splits[11], (SEQS, LEN, TOP), jnp.float32) ** level_of(splits[11], (SEQS, LEN, TOP), ((0, 8), (1, 16)), -0.2, 0.2)), 0.05, 1.0)
    w_gate = scatter_about(splits[12], (EXPERTS, D, DE), D ** -0.5, 0.125, ((0, 128),))
    w_up = scatter_about(splits[13], (EXPERTS, D, DE), D ** -0.5, 0.125, ((0, 128),))
    w_down = scatter_about(splits[14], (EXPERTS, DE, D), DE ** -0.5, 0.25, ((0, 128),))
    return {"queries": queries, "keys": keys, "values": values, "q_gain": q_gain, "k_gain": k_gain, "residual": residual, "out_weight": out_weight, "mix_gain": mix_gain, "ffn_gain": ffn_gain, "post_gain": post_gain, "expert_ids": expert_ids, "expert_gate": expert_gate, "w_gate": w_gate, "w_up": w_up, "w_down": w_down}


eps_norm = 1e-06
theta_base = 10000.0
block_rows = 512

def rms_scale(values):
    return values * lax.rsqrt(lax.optimization_barrier(jnp.mean(values * values, axis=-1, keepdims=True)) + eps_norm)

def rotate(field, gain):
    seq_len, head_count, head_size = field.shape
    values = rms_scale(field.astype(jnp.float32)) * gain
    positions = jnp.arange(seq_len, dtype=jnp.int32)
    row_index = (positions // GRID).astype(jnp.float32)
    col_index = (positions % GRID).astype(jnp.float32)
    pair_quarter = head_size // 4
    frequency = theta_base ** (-(4.0 * jnp.arange(pair_quarter, dtype=jnp.float32)) / head_size)
    angles = jnp.concatenate([row_index[:, None] * frequency, col_index[:, None] * frequency], axis=1)
    cosine_table = jnp.cos(angles)[:, None, :]
    sine_table = jnp.sin(angles)[:, None, :]
    paired = values.reshape(seq_len, head_count, head_size // 2, 2)
    even_part = paired[..., 0]
    odd_part = paired[..., 1]
    turned = jnp.stack([even_part * cosine_table - odd_part * sine_table, even_part * sine_table + odd_part * cosine_table], axis=-1)
    return turned.reshape(seq_len, head_count, head_size).astype(jnp.bfloat16)

def attend(q_turned, k_turned, v_rows):
    seq_len, q_count, head_size = q_turned.shape
    kv_count = k_turned.shape[1]
    group_size = q_count // kv_count
    k_float = k_turned.astype(jnp.float32)
    v_float = v_rows.astype(jnp.float32)

    def one_block(start):
        q_block = lax.dynamic_slice_in_dim(q_turned, start, block_rows, 0)
        q_block = q_block.reshape(block_rows, kv_count, group_size, head_size).astype(jnp.float32)
        scores = jnp.einsum('qkgd,skd->kgqs', q_block, k_float) * head_size ** (-0.5)
        row_max = lax.optimization_barrier(jnp.max(scores, axis=-1, keepdims=True))
        exp_scores = jnp.exp(scores - row_max)
        weights = (exp_scores / lax.optimization_barrier(jnp.sum(exp_scores, axis=-1, keepdims=True))).astype(jnp.bfloat16)
        summed = jnp.einsum('kgqs,skd->qkgd', weights.astype(jnp.float32), v_float)
        return summed.astype(jnp.bfloat16).reshape(block_rows, q_count * head_size)
    starts = jnp.arange(seq_len // block_rows, dtype=jnp.int32) * block_rows
    return lax.map(one_block, starts).reshape(seq_len, q_count * head_size)

def reference(queries, keys, values, q_gain, k_gain, residual, out_weight, mix_gain, ffn_gain, post_gain, expert_ids, expert_gate, w_gate, w_up, w_down):
    seq_count, seq_len, q_width = queries.shape
    head_size = q_gain.shape[0]

    def per_sequence(items):
        q_seq, k_seq, v_seq = items
        q_turned = rotate(q_seq.reshape(seq_len, -1, head_size), q_gain)
        k_turned = rotate(k_seq.reshape(seq_len, -1, head_size), k_gain)
        return attend(q_turned, k_turned, v_seq.reshape(seq_len, -1, head_size))
    attended = lax.map(per_sequence, (queries, keys, values)).reshape(-1, q_width)
    projected = jnp.dot(attended, out_weight, preferred_element_type=jnp.float32)
    first_res = (residual.reshape(-1, D).astype(jnp.float32) + rms_scale(projected) * mix_gain).astype(jnp.bfloat16)
    normed = (rms_scale(first_res.astype(jnp.float32)) * ffn_gain).astype(jnp.bfloat16)
    flat_ids = expert_ids.reshape(-1).astype(jnp.int32)
    flat_gate = expert_gate.reshape(-1)
    slot_count = N_SP * N_DP * CAP

    def per_expert(running_sum, number):
        matches = flat_ids == number
        picked = jnp.nonzero(matches, size=slot_count, fill_value=0)[0].astype(jnp.int32)
        live_mask = (jnp.arange(slot_count, dtype=jnp.int32) < jnp.sum(matches.astype(jnp.int32))).astype(jnp.float32)
        token_rows = (picked // TOP).astype(jnp.int32)
        inputs = normed[token_rows]
        gate_value = jnp.dot(inputs, w_gate[number], preferred_element_type=jnp.float32)
        up_value = jnp.dot(inputs, w_up[number], preferred_element_type=jnp.float32)
        hidden = (jax.nn.silu(gate_value) * up_value).astype(jnp.bfloat16)
        expert_out = jnp.dot(hidden, w_down[number], preferred_element_type=jnp.float32).astype(jnp.bfloat16)
        weight = flat_gate[picked] * live_mask
        return (running_sum.at[token_rows].add(weight[:, None] * expert_out.astype(jnp.float32)), None)
    expert_sum, _ = lax.scan(per_expert, jnp.zeros((normed.shape[0], D), jnp.float32), jnp.arange(EXPERTS, dtype=jnp.int32))
    result = (first_res.astype(jnp.float32) + rms_scale(expert_sum) * post_gain).astype(jnp.bfloat16)
    return result.reshape(seq_count, seq_len, D)
```

```python
import functools

import numpy as np
import jax
import jax.numpy as jnp
from jax import lax
from jax.experimental import pallas as pl
from jax.experimental.pallas import tpu as pltpu
from jax.sharding import PartitionSpec as P

MESH = pl.DeviceIdType.MESH
F32, BF16 = jnp.float32, jnp.bfloat16
EPS = 1e-06
GRID = 64
D = 2048
TOK = 128
SLOTS = 512

PARTS = (((0, 1, 2), 0, 640), ((1, 2, 0), 640, 640), ((2, 0, 1), 1280, 768))
PAIRS = ((0, 1), (1, 0))
NEAR = (1, 3, 2)
SIDES = tuple((k3, kc) for k3 in range(4) for kc in range(2) if (k3, kc) != (0, 0))


def tables():
    lane = np.arange(128) % 64
    pair = lane // 2
    freq = 10000.0 ** (-4.0 * (pair % 16) / 64.0)
    sign = np.where(lane % 2 == 0, -1.0, 1.0)
    row_lane = pair < 16
    rows = np.zeros((16, 8, 128), np.float32)
    for s in range(16):
        for i in range(2):
            ang = (2 * s + i) * freq
            rows[s, i] = np.where(row_lane, np.cos(ang), 0.0)
            rows[s, 2 + i] = np.where(row_lane, np.sin(ang) * sign, 0.0)
    ang = np.arange(64)[:, None] * freq[None, :]
    cols = np.stack(
        [np.where(row_lane, 0.0, np.cos(ang)), np.where(row_lane, 0.0, np.sin(ang) * sign)]
    ).astype(np.float32)
    return rows, cols


def rms(v):
    return v * lax.rsqrt(jnp.mean(v * v, axis=-1, keepdims=True) + EPS)


def kernel(
    q_ref, k_ref, v_ref, qg_ref, kg_ref, res_ref, wo_hbm, mix_ref, ffn_ref, post_ref,
    ids_ref, gate_ref, wg_hbm, wu_hbm, wd_hbm, rtab_ref, ctab_ref,
    out_ref,
    wo, wg, wu, wd, qp, kv, mx, acc, att, first, normed, disp, comb,
    outbox, inbox, mid, xs, ys, midr, inboxr, outr, hg, hu,
    wsem, gs, gr, f1s, f1r, f2s, f2r, f3s, f3r, r1s, r1r, r2s, r2r, r3s, r3r, own_sem,
):
    s = lax.axis_index("sp")
    d = lax.axis_index("dp")
    mine = (s // 4, s % 4, d // 2)
    core = d % 2

    def dev(axis, k, kc=0):
        p = list(mine)
        p[axis] = (p[axis] + k) % 4
        return (p[0] * 4 + p[1], p[2] * 2 + (core + kc) % 2)

    barrier = pltpu.get_barrier_semaphore()
    peers = [dev(a, k, kc) for a in range(3) for k in NEAR for kc in range(2)] + [dev(0, 0, 1)]
    for peer in peers:
        pl.semaphore_signal(barrier, 1, device_id=peer, device_id_type=MESH)

    weights = [
        pltpu.make_async_copy(src, dst, wsem.at[i])
        for i, (src, dst) in enumerate(
            ((wo_hbm, wo), (wg_hbm.at[0], wg), (wu_hbm.at[0], wu), (wd_hbm.at[0], wd))
        )
    ]
    for w in weights:
        w.start()

    lane = lax.broadcasted_iota(jnp.int32, (TOK, 128), 1)
    even = (lane % 2) == 0
    low = lane < 64
    seg = jnp.where(
        (lax.broadcasted_iota(jnp.int32, (128, 128), 0) // 64)
        == (lax.broadcasted_iota(jnp.int32, (128, 128), 1) // 64),
        1.0 / 64.0,
        0.0,
    ).astype(BF16)
    rt = rtab_ref[s]
    cos = jnp.concatenate([ctab_ref[0] + rt[0:1], ctab_ref[0] + rt[1:2]], axis=0)
    sin = jnp.concatenate([ctab_ref[1] + rt[2:3], ctab_ref[1] + rt[3:4]], axis=0)

    def turn(x, gain):
        x = x.astype(F32)
        sq = x * x
        hi = sq.astype(BF16)
        lo = (sq - hi.astype(F32)).astype(BF16)
        ms = jnp.dot(hi, seg, preferred_element_type=F32) + jnp.dot(
            lo, seg, preferred_element_type=F32
        )
        y = x * lax.rsqrt(ms + EPS) * gain
        swapped = jnp.where(even, pltpu.roll(y, 127, 1), pltpu.roll(y, 1, 1))
        return y * cos + swapped * sin

    kgain = jnp.concatenate([kg_ref[...], kg_ref[...]], axis=1)
    qgain = jnp.concatenate([qg_ref[...], qg_ref[...]], axis=1)
    for p in range(2):
        cols = slice(p * 128, (p + 1) * 128)
        kv[p, 0, :, 0:128] = turn(k_ref[0, :, cols], kgain).astype(BF16)
        kv[p, 0, :, 128:256] = v_ref[0, :, cols]
        kv[p, :, :, 256:384] = jnp.ones((16, TOK, 128), BF16)

    pl.semaphore_wait(barrier, len(peers))

    def hop(p, axis, k, src, dst):
        return pltpu.make_async_remote_copy(
            src_ref=kv.at[p, src, :, pl.ds(0, 256)],
            dst_ref=kv.at[p, dst, :, pl.ds(0, 256)],
            send_sem=gs.at[p, dst],
            recv_sem=gr.at[p, dst],
            device_id=dev(axis, k),
            device_id_type=MESH,
        )

    def gather_first(p, k1):
        return hop(p, PAIRS[p][0], k1, 0, k1)

    def gather_second(p, k2, k1):
        if k2 == 2:
            k = 1 if k1 < 2 else 3
            return hop(p, PAIRS[p][1], k, k * 4 + k1, 8 + k1)
        return hop(p, PAIRS[p][1], k2, k1, k2 * 4 + k1)

    for k1 in NEAR:
        for p in range(2):
            gather_first(p, k1).start()
    for k2 in (1, 3):
        for p in range(2):
            gather_second(p, k2, 0).start()

    for b in range(8):
        t = turn(q_ref[0, :, b * 128 : (b + 1) * 128], qgain).astype(BF16).astype(F32) * 0.125
        flip = pltpu.roll(t, 64, 1)
        p, pos, i = b // 4, (b // 2) % 2, (b % 4) * 2
        if pos == 0:
            a0, a1 = jnp.where(low, t, 0.0), jnp.where(low, flip, 0.0)
        else:
            a0, a1 = jnp.where(low, 0.0, flip), jnp.where(low, 0.0, t)
        qp[p, i * 128 : (i + 1) * 128] = a0.astype(BF16)
        qp[p, (i + 1) * 128 : (i + 2) * 128] = a1.astype(BF16)

    for k1 in NEAR:
        for p in range(2):
            gather_first(p, k1).wait_recv()
            for k2 in (1, 3):
                gather_second(p, k2, k1).start()

    tok_r = lax.broadcasted_iota(jnp.int32, (128, 128), 0)
    tok_c = lax.broadcasted_iota(jnp.int32, (128, 128), 1)
    before = (tok_r < tok_c).astype(F32).astype(BF16)
    ids = ids_ref[0].astype(F32)
    idt = [jnp.transpose(jnp.broadcast_to(ids[:, k : k + 1], (128, 128))) for k in range(2)]
    hot = [(t == tok_r.astype(F32)).astype(F32) for t in idt]
    cnt = [jnp.dot(h.astype(BF16), before, preferred_element_type=F32) for h in hot]
    cnt[1] = cnt[1] + jnp.sum(hot[0], axis=1, keepdims=True)
    rank = [jnp.sum(h * c, axis=0, keepdims=True).astype(jnp.int32) for h, c in zip(hot, cnt)]
    slot_row = lax.broadcasted_iota(jnp.int32, (SLOTS, 128), 0)
    slot_col = lax.broadcasted_iota(jnp.int32, (128, SLOTS), 1).astype(F32)
    for p, (axes, _, _) in enumerate(PARTS):
        slots = []
        for k in range(2):
            e = idt[k][0:1].astype(jnp.int32)
            at = (e // 32, (e // 8) % 4, (e // 2) % 4)
            rel = [(at[a] - mine[a] + 4) % 4 for a in axes]
            kc = (e % 2 + core) % 2
            slots.append(((rel[0] * 4 + rel[1]) * 4 + rel[2]) * 8 + kc * 4 + rank[k])
        disp[p] = ((slot_row == slots[0]) | (slot_row == slots[1])).astype(F32).astype(BF16)
        for k in range(2):
            col = jnp.transpose(jnp.broadcast_to(slots[k].astype(F32), (128, 128)))[:, 0:1]
            comb[p, k] = (slot_col == col).astype(F32).astype(BF16)

    def stripe(k2, fresh):
        for p in range(2):
            keys = kv[p, k2 * 4 : k2 * 4 + 4, :, 0:128].reshape(512, 128)
            vals = kv[p, k2 * 4 : k2 * 4 + 4, :, 128:384].reshape(512, 256)

            def rows(i, _):
                r = pl.ds(pl.multiple_of(i * 512, 512), 512)
                sc = lax.dot_general(
                    qp[p, r, :], keys, (((1,), (1,)), ((), ())), preferred_element_type=F32
                )
                top = jnp.max(sc, axis=1, keepdims=True)
                if not fresh:
                    old = mx[p, r, 0:1]
                    top = jnp.maximum(top, old)
                e = jnp.exp(sc - top).astype(BF16)
                o = jnp.dot(e, vals, preferred_element_type=F32)
                if not fresh:
                    o = o + acc[p, r, :] * jnp.exp(old - top)
                acc[p, r, :] = o
                mx[p, r, :] = jnp.broadcast_to(top, (512, 128))
                return 0

            lax.fori_loop(0, 2, rows, 0)

    stripe(0, True)
    for k1 in (0, 1, 2, 3):
        k2 = 1 if k1 < 2 else 3
        for p in range(2):
            gather_second(p, k2, k1).wait_recv()
            gather_second(p, 2, k1).start()
    for k2, rest in ((1, (2, 3)), (3, (0, 1))):
        for k1 in rest:
            for p in range(2):
                gather_second(p, k2, k1).wait_recv()
        stripe(k2, False)
    for k1 in range(4):
        for p in range(2):
            gather_second(p, 2, k1).wait_recv()
    stripe(2, False)

    for b in range(8):
        p, pos, i = b // 4, (b // 2) % 2, (b % 4) * 2
        o = []
        for j in (i, i + 1):
            r = slice(j * 128, (j + 1) * 128)
            o.append(acc[p, r, 0:128] / acc[p, r, 128:256])
        if pos == 0:
            a = jnp.where(low, o[0], pltpu.roll(o[1], 64, 1))
        else:
            a = jnp.where(low, pltpu.roll(o[0], 64, 1), o[1])
        att[:, b * 128 : (b + 1) * 128] = a.astype(BF16)

    weights[0].wait()
    projected = jnp.dot(att[...], wo[...], preferred_element_type=F32)
    fr = (res_ref[0].astype(F32) + rms(projected) * mix_ref[...]).astype(BF16)
    first[...] = fr
    normed[...] = (rms(fr.astype(F32)) * ffn_ref[...]).astype(BF16)

    def cols_of(p):
        return pl.ds(PARTS[p][1], PARTS[p][2])

    def canon(p, k2, k1, k3, kc):
        rel = dict(zip(PARTS[p][0], (k1, k2, k3)))
        return rel[1], rel[0], (rel[2] * 2 + kc) * 4

    def remote(src, dst, ss, rs, device):
        return pltpu.make_async_remote_copy(
            src_ref=src, dst_ref=dst, send_sem=ss, recv_sem=rs, device_id=device, device_id_type=MESH
        )

    def stage1(p, k1, back):
        axis = PARTS[p][0][0]
        c = cols_of(p)
        if back:
            return remote(inboxr.at[k1, :, c], outr.at[k1, :, c], r3s.at[p, k1], r3r.at[p, k1], dev(axis, 4 - k1))
        return remote(outbox.at[k1, :, c], inbox.at[k1, :, c], f1s.at[p, k1], f1r.at[p, k1], dev(axis, k1))

    def stage2(p, k2, k1, back):
        axis = PARTS[p][0][1]
        c = cols_of(p)
        if back:
            dst = (outr if k1 == 0 else inboxr).at[k1, pl.ds(k2 * 32, 32), c]
            return remote(midr.at[k2, k1, :, c], dst, r2s.at[p, k2, k1], r2r.at[p, k2, k1], dev(axis, 4 - k2))
        src = (outbox if k1 == 0 else inbox).at[k1, pl.ds(k2 * 32, 32), c]
        return remote(src, mid.at[k2, k1, :, c], f2s.at[p, k2, k1], f2r.at[p, k2, k1], dev(axis, k2))

    def hold(p, k2, k1, k3, kc, back):
        r = k3 * 8 + kc * 4
        c = cols_of(p)
        if k2 > 0:
            return (midr if back else mid).at[k2, k1, pl.ds(r, 4), c]
        if k1 > 0:
            return (inboxr if back else inbox).at[k1, pl.ds(r, 4), c]
        return (outr if back else outbox).at[0, pl.ds(r, 4), c]

    def stage3(p, k2, k1, k3, kc, back):
        axis = PARTS[p][0][2]
        ky, kz, r = canon(p, k2, k1, k3, kc)
        n = k3 * 2 + kc
        here = hold(p, k2, k1, k3, kc, back)
        c = cols_of(p)
        if n == 0:
            if back:
                return pltpu.make_async_copy(ys.at[ky, kz, pl.ds(r, 4), c], here, own_sem.at[1, p, k2, k1])
            return pltpu.make_async_copy(here, xs.at[ky, kz, pl.ds(r, 4), c], own_sem.at[0, p, k2, k1])
        if back:
            return remote(ys.at[ky, kz, pl.ds(r, 4), c], here, r1s.at[p, k2, k1, n], r1r.at[p, k2, k1, n], dev(axis, 4 - k3, kc))
        return remote(here, xs.at[ky, kz, pl.ds(r, 4), c], f3s.at[p, k2, k1, n], f3r.at[p, k2, k1, n], dev(axis, k3, kc))

    ALL3 = ((0, 0),) + tuple((k3, kc) for k3 in NEAR for kc in range(2)) + ((0, 1),)

    def fan(p, k2, k1):
        for k3, kc in ALL3:
            stage3(p, k2, k1, k3, kc, False).start()

    for p in range(3):
        c = slice(PARTS[p][1], PARTS[p][1] + PARTS[p][2])
        outbox[:, :, c] = (
            jnp.dot(disp[p], normed[:, c], preferred_element_type=F32)
            .astype(BF16)
            .reshape(4, 128, PARTS[p][2])
        )
        for k1 in NEAR:
            stage1(p, k1, False).start()
        for k2 in NEAR:
            stage2(p, k2, 0, False).start()
    for p in range(3):
        fan(p, 0, 0)
    for k1 in NEAR:
        for p in range(3):
            stage1(p, k1, False).wait_recv()
            for k2 in NEAR:
                stage2(p, k2, k1, False).start()
            fan(p, 0, k1)
    for k1 in (0,) + NEAR:
        for k2 in NEAR:
            for p in range(3):
                stage2(p, k2, k1, False).wait_recv()
                fan(p, k2, k1)

    weights[1].wait()
    weights[2].wait()
    for p in range(3):
        for k2 in range(4):
            for k1 in range(4):
                for k3 in range(4):
                    for kc in range(2):
                        cp = stage3(p, k2, k1, k3, kc, False)
                        if (k3, kc) == (0, 0):
                            cp.wait()
                        else:
                            cp.wait_recv()
        c = slice(PARTS[p][1], PARTS[p][1] + PARTS[p][2])

        def up(i, _):
            x = xs[i, :, :, c].reshape(128, PARTS[p][2])
            g = jnp.dot(x, wg[c, :], preferred_element_type=F32)
            u = jnp.dot(x, wu[c, :], preferred_element_type=F32)
            if p > 0:
                g, u = g + hg[i], u + hu[i]
            hg[i] = g
            hu[i] = u
            return 0

        lax.fori_loop(0, 4, up, 0)

    weights[3].wait()
    hidden = (jax.nn.silu(hg[...]) * hu[...]).astype(BF16).reshape(SLOTS, 512)
    for p in range(3):
        c = slice(PARTS[p][1], PARTS[p][1] + PARTS[p][2])
        ys[:, :, :, c] = (
            jnp.dot(hidden, wd[:, c], preferred_element_type=F32)
            .astype(BF16)
            .reshape(4, 4, 32, PARTS[p][2])
        )
        for k2 in NEAR + (0,):
            for k1 in NEAR + (0,):
                for k3, kc in ALL3:
                    stage3(p, k2, k1, k3, kc, True).start()

    def arrived3(p, k2, k1):
        for k3, kc in ALL3:
            cp = stage3(p, k2, k1, k3, kc, True)
            if (k3, kc) == (0, 0):
                cp.wait()
            else:
                cp.wait_recv()

    for k2 in NEAR:
        for k1 in NEAR + (0,):
            for p in range(3):
                arrived3(p, k2, k1)
                stage2(p, k2, k1, True).start()
    for k1 in NEAR:
        for p in range(3):
            arrived3(p, 0, k1)
            for k2 in NEAR:
                stage2(p, k2, k1, True).wait_recv()
            stage1(p, k1, True).start()
    for p in range(3):
        arrived3(p, 0, 0)
        for k2 in NEAR:
            stage2(p, k2, 0, True).wait_recv()

    g0, g1 = gate_ref[0, :, 0:1], gate_ref[0, :, 1:2]
    sums = []
    for p in range(3):
        for k1 in NEAR:
            stage1(p, k1, True).wait_recv()
        c = slice(PARTS[p][1], PARTS[p][1] + PARTS[p][2])
        back = outr[:, :, c].reshape(SLOTS, PARTS[p][2])
        a0 = jnp.dot(comb[p, 0], back, preferred_element_type=F32)
        a1 = jnp.dot(comb[p, 1], back, preferred_element_type=F32)
        sums.append(g0 * a0 + g1 * a1)
    total = jnp.concatenate(sums, axis=1)
    out_ref[0] = (first[...].astype(F32) + rms(total) * post_ref[...]).astype(BF16)

    for p in range(2):
        for k1 in NEAR:
            gather_first(p, k1).wait_send()
        for k2 in NEAR:
            for k1 in range(4):
                gather_second(p, k2, k1).wait_send()
    for p in range(3):
        for back in (False, True):
            for k1 in NEAR:
                stage1(p, k1, back).wait_send()
            for k2 in NEAR:
                for k1 in range(4):
                    stage2(p, k2, k1, back).wait_send()
            for k2 in range(4):
                for k1 in range(4):
                    for k3, kc in SIDES:
                        stage3(p, k2, k1, k3, kc, back).wait_send()


def shards(
    queries, keys, values, q_gain, k_gain, residual, out_weight, mix_gain, ffn_gain, post_gain,
    expert_ids, expert_gate, w_gate, w_up, w_down,
):
    rows, cols = tables()
    vm = pl.BlockSpec(memory_space=pltpu.VMEM)
    hbm = pl.BlockSpec(memory_space=pl.ANY)
    sem = pltpu.SemaphoreType.DMA
    box = pltpu.VMEM((4, 128, D), BF16)
    deep = pltpu.VMEM((4, 4, 32, D), BF16)
    return pl.pallas_call(
        kernel,
        out_shape=jax.ShapeDtypeStruct((1, TOK, D), BF16),
        in_specs=[vm, vm, vm, vm, vm, vm, hbm, vm, vm, vm, vm, vm, hbm, hbm, hbm, vm, vm],
        out_specs=vm,
        scratch_shapes=[
            pltpu.VMEM((1024, D), BF16),
            pltpu.VMEM((D, 512), BF16),
            pltpu.VMEM((D, 512), BF16),
            pltpu.VMEM((512, D), BF16),
            pltpu.VMEM((2, 1024, 128), BF16),
            pltpu.VMEM((2, 16, TOK, 384), BF16),
            pltpu.VMEM((2, 1024, 128), F32),
            pltpu.VMEM((2, 1024, 256), F32),
            pltpu.VMEM((TOK, 1024), BF16),
            pltpu.VMEM((TOK, D), BF16),
            pltpu.VMEM((TOK, D), BF16),
            pltpu.VMEM((3, SLOTS, 128), BF16),
            pltpu.VMEM((3, 2, 128, SLOTS), BF16),
            box, box, deep, deep, deep, deep, box, box,
            pltpu.VMEM((4, 128, 512), F32),
            pltpu.VMEM((4, 128, 512), F32),
            sem((4,)),
            sem((2, 16)), sem((2, 16)),
            sem((3, 4)), sem((3, 4)),
            sem((3, 4, 4)), sem((3, 4, 4)),
            sem((3, 4, 4, 8)), sem((3, 4, 4, 8)),
            sem((3, 4, 4, 8)), sem((3, 4, 4, 8)),
            sem((3, 4, 4)), sem((3, 4, 4)),
            sem((3, 4)), sem((3, 4)),
            sem((2, 3, 4, 4)),
        ],
        compiler_params=pltpu.CompilerParams(
            collective_id=0, has_side_effects=True, vmem_limit_bytes=60 * 2**20
        ),
        name="layer",
    )(
        queries, keys, values, q_gain[None], k_gain[None], residual, out_weight,
        mix_gain[None], ffn_gain[None], post_gain[None], expert_ids, expert_gate,
        w_gate, w_up, w_down, jnp.asarray(rows), jnp.asarray(cols),
    )


def solution(mesh):
    return jax.shard_map(
        shards,
        mesh=mesh,
        in_specs=(
            P("dp", "sp", None), P("dp", "sp", None), P("dp", "sp", None), P(), P(),
            P("dp", "sp", None), P(), P(), P(), P(),
            P("dp", "sp", None), P("dp", "sp", None),
            P(("sp", "dp"), None, None), P(("sp", "dp"), None, None), P(("sp", "dp"), None, None),
        ),
        out_specs=P("dp", "sp", None),
        check_vma=False,
    )
```

```python
import functools

import numpy as np
import jax
import jax.numpy as jnp
from jax import lax
from jax.experimental import pallas as pl
from jax.experimental.pallas import tpu as pltpu
from jax.sharding import PartitionSpec as P

MESH = pl.DeviceIdType.MESH
F32, BF16 = jnp.float32, jnp.bfloat16
EPS = 1e-06
GRID = 64
D = 2048
TOK = 128
SLOTS = 512
ROWS = 256

PARTS = (
    ((0, 1, 2), 0, 384), ((1, 2, 0), 384, 384), ((2, 0, 1), 768, 384),
    ((0, 1, 2), 1152, 256), ((1, 2, 0), 1408, 256), ((2, 0, 1), 1664, 384),
)
WAVES = ((0, 1, 2), (3, 4, 5))
NP = len(PARTS)
PLACE = {0: 0, 1: 1, 3: 2, 2: 3}
PAIRS = ((0, 1), (1, 0))
NEAR = (2, 1, 3)


def tables():
    lane = np.arange(128) % 64
    pair = lane // 2
    freq = 10000.0 ** (-4.0 * (pair % 16) / 64.0)
    sign = np.where(lane % 2 == 0, -1.0, 1.0)
    row_lane = pair < 16
    rows = np.zeros((16, 8, 128), np.float32)
    for s in range(16):
        for i in range(2):
            ang = (2 * s + i) * freq
            rows[s, i] = np.where(row_lane, np.cos(ang), 0.0)
            rows[s, 2 + i] = np.where(row_lane, np.sin(ang) * sign, 0.0)
    ang = np.arange(64)[:, None] * freq[None, :]
    cols = np.stack(
        [np.where(row_lane, 0.0, np.cos(ang)), np.where(row_lane, 0.0, np.sin(ang) * sign)]
    ).astype(np.float32)
    return rows, cols


def rms(v):
    return v * lax.rsqrt(jnp.mean(v * v, axis=-1, keepdims=True) + EPS)


def kernel(
    q_ref, k_ref, v_ref, qg_ref, kg_ref, res_ref, wo_hbm, mix_ref, ffn_ref, post_ref,
    ids_ref, gate_ref, wg_hbm, wu_hbm, wd_hbm, rtab_ref, ctab_ref,
    out_ref,
    wo, wg, wu, wd, qp, kv, mx, acc, att, first, normed, disp, comb,
    outbox, inbox, mid, xs, ys, midr, inboxr, outr, hg, hu,
    wsem, gs, gr, f1r, f2r, f3r, r1r, r2r, r3r, sent,
):
    s = lax.axis_index("sp")
    d = lax.axis_index("dp")
    mine = (s // 4, s % 4, d // 2)
    core = d % 2

    def dev(axis, k, kc=0):
        p = list(mine)
        p[axis] = (p[axis] + k) % 4
        return (p[0] * 4 + p[1], p[2] * 2 + (core + kc) % 2)

    barrier = pltpu.get_barrier_semaphore()
    peers = [dev(a, k, kc) for a in range(3) for k in NEAR for kc in range(2)] + [dev(0, 0, 1)]
    for peer in peers:
        pl.semaphore_signal(barrier, 1, device_id=peer, device_id_type=MESH)

    weights = [
        pltpu.make_async_copy(src, dst, wsem.at[i])
        for i, (src, dst) in enumerate(
            ((wo_hbm, wo), (wg_hbm.at[0], wg), (wu_hbm.at[0], wu), (wd_hbm.at[0], wd))
        )
    ]
    for w in weights:
        w.start()

    lane = lax.broadcasted_iota(jnp.int32, (TOK, 128), 1)
    even = (lane % 2) == 0
    low = lane < 64
    seg = jnp.where(
        (lax.broadcasted_iota(jnp.int32, (128, 128), 0) // 64)
        == (lax.broadcasted_iota(jnp.int32, (128, 128), 1) // 64),
        1.0 / 64.0,
        0.0,
    ).astype(BF16)
    rt = rtab_ref[s]
    cos = jnp.concatenate([ctab_ref[0] + rt[0:1], ctab_ref[0] + rt[1:2]], axis=0)
    sin = jnp.concatenate([ctab_ref[1] + rt[2:3], ctab_ref[1] + rt[3:4]], axis=0)

    def turn(x, gain):
        x = x.astype(F32)
        sq = x * x
        hi = sq.astype(BF16)
        lo = (sq - hi.astype(F32)).astype(BF16)
        ms = jnp.dot(hi, seg, preferred_element_type=F32) + jnp.dot(
            lo, seg, preferred_element_type=F32
        )
        y = x * lax.rsqrt(ms + EPS) * gain
        swapped = jnp.where(even, pltpu.roll(y, 127, 1), pltpu.roll(y, 1, 1))
        return y * cos + swapped * sin

    kgain = jnp.concatenate([kg_ref[...], kg_ref[...]], axis=1)
    qgain = jnp.concatenate([qg_ref[...], qg_ref[...]], axis=1)
    for p in range(2):
        cols = slice(p * 128, (p + 1) * 128)
        kv[p, 0, :, 0:128] = turn(k_ref[0, :, cols], kgain).astype(BF16)
        kv[p, 0, :, 128:256] = v_ref[0, :, cols]
        kv[p, :, :, 256:384] = jnp.ones((16, TOK, 128), BF16)

    for b in range(8):
        t = turn(q_ref[0, :, b * 128 : (b + 1) * 128], qgain).astype(BF16).astype(F32) * 0.125
        flip = pltpu.roll(t, 64, 1)
        p, pos, i = b // 4, (b // 2) % 2, (b % 4) * 2
        if pos == 0:
            a0, a1 = jnp.where(low, t, 0.0), jnp.where(low, flip, 0.0)
        else:
            a0, a1 = jnp.where(low, 0.0, flip), jnp.where(low, 0.0, t)
        qp[p, i * 128 : (i + 1) * 128] = a0.astype(BF16)
        qp[p, (i + 1) * 128 : (i + 2) * 128] = a1.astype(BF16)

    pl.semaphore_wait(barrier, len(peers))

    def hop(p, axis, k, src, dst):
        return pltpu.make_async_remote_copy(
            src_ref=kv.at[p, src, :, pl.ds(0, 256)],
            dst_ref=kv.at[p, dst, :, pl.ds(0, 256)],
            send_sem=gs.at[p, dst // 4],
            recv_sem=gr.at[p, dst],
            device_id=dev(axis, k),
            device_id_type=MESH,
        )

    def gather_first(p, k1):
        return hop(p, PAIRS[p][0], k1, 0, k1)

    def gather_second(p, k2, k1):
        if k2 == 2:
            k = 1 if k1 < 2 else 3
            return hop(p, PAIRS[p][1], k, PLACE[k] * 4 + k1, PLACE[2] * 4 + k1)
        return hop(p, PAIRS[p][1], k2, k1, PLACE[k2] * 4 + k1)

    for k1 in NEAR:
        for p in range(2):
            gather_first(p, k1).start()
    for k2 in (1, 3):
        for p in range(2):
            gather_second(p, k2, 0).start()

    for k1 in NEAR:
        for p in range(2):
            gather_first(p, k1).wait_recv()
            for k2 in (1, 3):
                gather_second(p, k2, k1).start()

    tok_r = lax.broadcasted_iota(jnp.int32, (128, 128), 0)
    tok_c = lax.broadcasted_iota(jnp.int32, (128, 128), 1)
    before = (tok_r < tok_c).astype(F32).astype(BF16)
    idt = [ids_ref[k : k + 1, :] for k in range(2)]
    hot = [(t == tok_r).astype(F32) for t in idt]
    cnt = [jnp.dot(h.astype(BF16), before, preferred_element_type=F32) for h in hot]
    cnt[1] = cnt[1] + jnp.sum(hot[0], axis=1, keepdims=True)
    rank = [jnp.sum(h * c, axis=0, keepdims=True).astype(jnp.int32) for h, c in zip(hot, cnt)]
    slot_row = lax.broadcasted_iota(jnp.int32, (SLOTS, 128), 0)
    slot_col = lax.broadcasted_iota(jnp.int32, (128, SLOTS), 1).astype(F32)
    for p, (axes, _, _) in enumerate(PARTS[:3]):
        slots = []
        for k in range(2):
            e = idt[k]
            at = (e // 32, (e // 8) % 4, (e // 2) % 4)
            rel = [(at[a] - mine[a] + 4) % 4 for a in axes]
            kc = (e % 2 + core) % 2
            slots.append(((rel[0] * 4 + rel[1]) * 4 + rel[2]) * 8 + kc * 4 + rank[k])
        disp[p] = ((slot_row == slots[0]) | (slot_row == slots[1])).astype(F32).astype(BF16)
        for k in range(2):
            col = jnp.transpose(jnp.broadcast_to(slots[k].astype(F32), (128, 128)))[:, 0:1]
            comb[p, k] = (slot_col == col).astype(F32).astype(BF16)

    def stripe(first_place, count, fresh):
        for p in range(2):
            span = slice(first_place * 4, (first_place + count) * 4)
            n = count * 512
            keys = kv[p, span, :, 0:128].reshape(n, 128)
            vals = kv[p, span, :, 128:384].reshape(n, 256)
            for i in range(1024 // ROWS):
                r = slice(i * ROWS, (i + 1) * ROWS)
                sc = lax.dot_general(
                    qp[p, r, :], keys, (((1,), (1,)), ((), ())), preferred_element_type=F32
                )
                top = jnp.broadcast_to(jnp.max(sc, axis=1, keepdims=True), (ROWS, 128))
                if not fresh:
                    old = mx[p, r, :]
                    top = jnp.maximum(top, old)
                    fade = jnp.exp(old - top)
                mx[p, r, :] = top
                e = jnp.exp(sc - jnp.concatenate([top] * (n // 128), axis=1)).astype(BF16)
                o = jnp.dot(e, vals, preferred_element_type=F32)
                if not fresh:
                    o = o + acc[p, r, :] * jnp.concatenate([fade, fade], axis=1)
                acc[p, r, :] = o

    stripe(0, 1, True)
    for k1 in (0, 1, 2, 3):
        k2 = 1 if k1 < 2 else 3
        for p in range(2):
            gather_second(p, k2, k1).wait_recv()
            gather_second(p, 2, k1).start()
    for k2, rest in ((1, (2, 3)), (3, (0, 1))):
        for k1 in rest:
            for p in range(2):
                gather_second(p, k2, k1).wait_recv()
    stripe(1, 2, False)
    for k1 in range(4):
        for p in range(2):
            gather_second(p, 2, k1).wait_recv()
    stripe(3, 1, False)

    for b in range(8):
        p, pos, i = b // 4, (b // 2) % 2, (b % 4) * 2
        o = []
        for j in (i, i + 1):
            r = slice(j * 128, (j + 1) * 128)
            o.append(acc[p, r, 0:128] / acc[p, r, 128:256])
        if pos == 0:
            a = jnp.where(low, o[0], pltpu.roll(o[1], 64, 1))
        else:
            a = jnp.where(low, pltpu.roll(o[0], 64, 1), o[1])
        att[:, b * 128 : (b + 1) * 128] = a.astype(BF16)

    weights[0].wait()
    projected = jnp.dot(att[...], wo[...], preferred_element_type=F32)
    fr = (res_ref[0].astype(F32) + rms(projected) * mix_ref[...]).astype(BF16)
    first[...] = fr
    normed[...] = (rms(fr.astype(F32)) * ffn_ref[...]).astype(BF16)

    def cols_of(p):
        return pl.ds(PARTS[p][1], PARTS[p][2])

    def canon(p, k2, k1, k3, kc):
        rel = dict(zip(PARTS[p][0], (k1, k2, k3)))
        return rel[1], rel[0], (rel[2] * 2 + kc) * 4

    def remote(src, dst, ss, rs, device):
        return pltpu.make_async_remote_copy(
            src_ref=src, dst_ref=dst, send_sem=ss, recv_sem=rs, device_id=device, device_id_type=MESH
        )

    def stage1(p, k1, back):
        axis = PARTS[p][0][0]
        c = cols_of(p)
        if back:
            return remote(inboxr.at[k1, :, c], outr.at[k1, :, c], sent.at[p, 5], r3r.at[p], dev(axis, 4 - k1))
        return remote(outbox.at[k1, :, c], inbox.at[k1, :, c], sent.at[p, 0], f1r.at[p, k1 - 1], dev(axis, k1))

    def stage2(p, k2, k1, back):
        axis = PARTS[p][0][1]
        c = cols_of(p)
        if back:
            dst = (outr if k1 == 0 else inboxr).at[k1, pl.ds(k2 * 32, 32), c]
            return remote(midr.at[k2, k1, :, c], dst, sent.at[p, 4], r2r.at[p, k1], dev(axis, 4 - k2))
        src = (outbox if k1 == 0 else inbox).at[k1, pl.ds(k2 * 32, 32), c]
        return remote(src, mid.at[k2, k1, :, c], sent.at[p, 1], f2r.at[p, k1], dev(axis, k2))

    def hold(p, k2, k1, k3, kc, back):
        r = k3 * 8 + kc * 4
        c = cols_of(p)
        if k2 > 0:
            return (midr if back else mid).at[k2, k1, pl.ds(r, 4), c]
        if k1 > 0:
            return (inboxr if back else inbox).at[k1, pl.ds(r, 4), c]
        return (outr if back else outbox).at[0, pl.ds(r, 4), c]

    def stage3(p, k2, k1, k3, kc, back):
        axis = PARTS[p][0][2]
        ky, kz, r = canon(p, k2, k1, k3, kc)
        n = k3 * 2 + kc
        here = hold(p, k2, k1, k3, kc, back)
        c = cols_of(p)
        far = xs.at[ky, kz, pl.ds(r, 4), c] if not back else ys.at[ky, kz, pl.ds(r, 4), c]
        if n == 0:
            if back:
                return pltpu.make_async_copy(far, here, r1r.at[p, k2])
            return pltpu.make_async_copy(here, far, f3r.at[p])
        if back:
            return remote(far, here, sent.at[p, 3], r1r.at[p, k2], dev(axis, 4 - k3, kc))
        return remote(here, far, sent.at[p, 2], f3r.at[p], dev(axis, k3, kc))

    def drain(ref, sem):
        pltpu.make_async_copy(ref, ref, sem).wait()

    ALL3 = ((0, 0),) + tuple((k3, kc) for k3 in NEAR for kc in range(2)) + ((0, 1),)

    def fan(p, k2, k1):
        for k3, kc in ALL3:
            stage3(p, k2, k1, k3, kc, False).start()

    for p in range(NP):
        c = slice(PARTS[p][1], PARTS[p][1] + PARTS[p][2])
        outbox[:, :, c] = (
            jnp.dot(disp[p % 3], normed[:, c], preferred_element_type=F32)
            .astype(BF16)
            .reshape(4, 128, PARTS[p][2])
        )
        for k1 in NEAR:
            stage1(p, k1, False).start()
        for k2 in NEAR:
            stage2(p, k2, 0, False).start()
    for p in range(NP):
        fan(p, 0, 0)
    for wave in WAVES:
        for k1 in (1, 3, 2):
            for p in wave:
                drain(inbox.at[k1, :, cols_of(p)], f1r.at[p, k1 - 1])
                for k2 in NEAR:
                    stage2(p, k2, k1, False).start()
                fan(p, 0, k1)
    for wave in WAVES:
        for k1 in (0, 1, 3, 2):
            for p in wave:
                drain(mid.at[pl.ds(1, 3), k1, :, cols_of(p)], f2r.at[p, k1])
                for k2 in NEAR:
                    fan(p, k2, k1)

    weights[1].wait()
    weights[2].wait()
    for p in range(NP):
        drain(xs.at[:, :, :, cols_of(p)], f3r.at[p])
        c = slice(PARTS[p][1], PARTS[p][1] + PARTS[p][2])

        def up(i, _):
            x = xs[i, :, :, c].reshape(128, PARTS[p][2])
            g = jnp.dot(x, wg[c, :], preferred_element_type=F32)
            u = jnp.dot(x, wu[c, :], preferred_element_type=F32)
            if p > 0:
                g, u = g + hg[i], u + hu[i]
            hg[i] = g
            hu[i] = u
            return 0

        lax.fori_loop(0, 4, up, 0)

    weights[3].wait()
    hidden = (jax.nn.silu(hg[...]) * hu[...]).astype(BF16).reshape(SLOTS, 512)
    for p in range(NP):
        c = slice(PARTS[p][1], PARTS[p][1] + PARTS[p][2])
        ys[:, :, :, c] = (
            jnp.dot(hidden, wd[:, c], preferred_element_type=F32)
            .astype(BF16)
            .reshape(4, 4, 32, PARTS[p][2])
        )
        for k2 in NEAR + (0,):
            for k1 in NEAR + (0,):
                for k3, kc in ALL3:
                    stage3(p, k2, k1, k3, kc, True).start()

    for wave in WAVES:
        for k2 in NEAR:
            for p in wave:
                drain(midr.at[k2, :, :, cols_of(p)], r1r.at[p, k2])
                for k1 in (2, 1, 3, 0):
                    stage2(p, k2, k1, True).start()
        for p in wave:
            drain(midr.at[0, :, :, cols_of(p)], r1r.at[p, 0])
    for wave in WAVES:
        for k1 in NEAR:
            for p in wave:
                drain(inboxr.at[k1, pl.ds(32, 96), cols_of(p)], r2r.at[p, k1])
                stage1(p, k1, True).start()
        for p in wave:
            drain(outr.at[0, pl.ds(32, 96), cols_of(p)], r2r.at[p, 0])

    g0, g1 = [jnp.transpose(jnp.broadcast_to(gate_ref[k : k + 1, :], (128, 128))) for k in range(2)]
    sums = []
    for p in range(NP):
        drain(outr.at[pl.ds(1, 3), :, cols_of(p)], r3r.at[p])
        c = slice(PARTS[p][1], PARTS[p][1] + PARTS[p][2])
        back = outr[:, :, c].reshape(SLOTS, PARTS[p][2])
        a0 = jnp.dot(comb[p % 3, 0], back, preferred_element_type=F32)
        a1 = jnp.dot(comb[p % 3, 1], back, preferred_element_type=F32)
        wide = PARTS[p][2] // 128
        sums.append(jnp.concatenate([g0] * wide, axis=1) * a0 + jnp.concatenate([g1] * wide, axis=1) * a1)
    total = jnp.concatenate(sums, axis=1)
    out_ref[0] = (first[...].astype(F32) + rms(total) * post_ref[...]).astype(BF16)

    for p in range(2):
        drain(kv.at[p, pl.ds(0, 3), :, pl.ds(0, 256)], gs.at[p, 0])
        for i in range(1, 4):
            drain(kv.at[p, pl.ds(0, 4), :, pl.ds(0, 256)], gs.at[p, i])
    for p in range(NP):
        c = cols_of(p)
        for i in (0, 1, 4, 5):
            drain(outbox.at[pl.ds(1, 3), :, c], sent.at[p, i])
        for i in (2, 3):
            drain(outbox.at[:, pl.ds(0, 112), c], sent.at[p, i])


def shards(
    queries, keys, values, q_gain, k_gain, residual, out_weight, mix_gain, ffn_gain, post_gain,
    expert_ids, expert_gate, w_gate, w_up, w_down,
):
    rows, cols = tables()
    vm = pl.BlockSpec(memory_space=pltpu.VMEM)
    hbm = pl.BlockSpec(memory_space=pl.ANY)
    sem = pltpu.SemaphoreType.DMA
    box = pltpu.VMEM((4, 128, D), BF16)
    deep = pltpu.VMEM((4, 4, 32, D), BF16)
    return pl.pallas_call(
        kernel,
        out_shape=jax.ShapeDtypeStruct((1, TOK, D), BF16),
        in_specs=[vm, vm, vm, vm, vm, vm, hbm, vm, vm, vm, vm, vm, hbm, hbm, hbm, vm, vm],
        out_specs=vm,
        scratch_shapes=[
            pltpu.VMEM((1024, D), BF16),
            pltpu.VMEM((D, 512), BF16),
            pltpu.VMEM((D, 512), BF16),
            pltpu.VMEM((512, D), BF16),
            pltpu.VMEM((2, 1024, 128), BF16),
            pltpu.VMEM((2, 16, TOK, 384), BF16),
            pltpu.VMEM((2, 1024, 128), F32),
            pltpu.VMEM((2, 1024, 256), F32),
            pltpu.VMEM((TOK, 1024), BF16),
            pltpu.VMEM((TOK, D), BF16),
            pltpu.VMEM((TOK, D), BF16),
            pltpu.VMEM((3, SLOTS, 128), BF16),
            pltpu.VMEM((3, 2, 128, SLOTS), BF16),
            box, box, deep, deep, deep, deep, box, box,
            pltpu.VMEM((4, 128, 512), F32),
            pltpu.VMEM((4, 128, 512), F32),
            sem((4,)),
            sem((2, 4)), sem((2, 16)),
            sem((NP, 3)), sem((NP, 4)), sem((NP,)),
            sem((NP, 4)), sem((NP, 4)), sem((NP,)),
            sem((NP, 6)),
        ],
        compiler_params=pltpu.CompilerParams(
            collective_id=0, has_side_effects=True, vmem_limit_bytes=60 * 2**20
        ),
        name="layer",
    )(
        queries, keys, values, q_gain[None], k_gain[None], residual, out_weight,
        mix_gain[None], ffn_gain[None], post_gain[None], expert_ids[0].T, expert_gate[0].T,
        w_gate, w_up, w_down, jnp.asarray(rows), jnp.asarray(cols),
    )


def solution(mesh):
    return jax.shard_map(
        shards,
        mesh=mesh,
        in_specs=(
            P("dp", "sp", None), P("dp", "sp", None), P("dp", "sp", None), P(), P(),
            P("dp", "sp", None), P(), P(), P(), P(),
            P("dp", "sp", None), P("dp", "sp", None),
            P(("sp", "dp"), None, None), P(("sp", "dp"), None, None), P(("sp", "dp"), None, None),
        ),
        out_specs=P("dp", "sp", None),
        check_vma=False,
    )
```

```python
import functools

import numpy as np
import jax
import jax.numpy as jnp
from jax import lax
from jax.experimental import pallas as pl
from jax.experimental.pallas import tpu as pltpu
from jax.sharding import PartitionSpec as P

MESH = pl.DeviceIdType.MESH
F32, BF16 = jnp.float32, jnp.bfloat16
EPS = 1e-06
GRID = 64
D = 2048
TOK = 128
SLOTS = 512
ROWS = 256
LIMIT = 60 * 2**20

PARTS = (((0, 1, 2), 0, 640), ((1, 2, 0), 640, 640), ((2, 0, 1), 1280, 768))
UNITS = tuple((w, p) for w in range(2) for p in range(3))
PLACE = {0: 0, 1: 1, 3: 2, 2: 3}
PAIRS = ((0, 1), (1, 0))
NEAR = (2, 1, 3)


def tables():
    lane = np.arange(128) % 64
    pair = lane // 2
    freq = 10000.0 ** (-4.0 * (pair % 16) / 64.0)
    sign = np.where(lane % 2 == 0, -1.0, 1.0)
    row_lane = pair < 16
    rows = np.zeros((16, 8, 128), np.float32)
    for s in range(16):
        for i in range(2):
            ang = (2 * s + i) * freq
            rows[s, i] = np.where(row_lane, np.cos(ang), 0.0)
            rows[s, 2 + i] = np.where(row_lane, np.sin(ang) * sign, 0.0)
    ang = np.arange(64)[:, None] * freq[None, :]
    cols = np.stack(
        [np.where(row_lane, 0.0, np.cos(ang)), np.where(row_lane, 0.0, np.sin(ang) * sign)]
    ).astype(np.float32)
    return rows, cols


def rms(v):
    return v * lax.rsqrt(jnp.mean(v * v, axis=-1, keepdims=True) + EPS)


def kernel(
    k_hbm, v_hbm, kg_hbm, rtab_hbm, ctab_hbm, q_hbm, qg_hbm, ids_hbm, gate_hbm, res_hbm,
    mix_hbm, ffn_hbm, post_hbm, wo_hbm, wg_hbm, wu_hbm, wd_hbm,
    out_ref,
    k_ref, v_ref, kg_ref, rtab_ref, ctab_ref, q_ref, qg_ref, ids_ref, gate_ref, res_ref,
    mix_ref, ffn_ref, post_ref,
    wo, wg, wu, wd, qp, kv, mx, acc, att, first, normed, disp, comb,
    outbox, inbox, mid, xs, ys, midr, inboxr, outr, tot,
    wsem, gs, gr, f1r, f2r, f3r, r1r, r1z, r2r, r3r, sent,
):
    s = lax.axis_index("sp")
    d = lax.axis_index("dp")
    mine = (s // 4, s % 4, d // 2)
    core = d % 2

    def dev(axis, k, kc=0):
        p = list(mine)
        p[axis] = (p[axis] + k) % 4
        return (p[0] * 4 + p[1], p[2] * 2 + (core + kc) % 2)

    def drain(ref, sem):
        pltpu.make_async_copy(ref, ref, sem).wait()

    barrier = pltpu.get_barrier_semaphore()
    peers = [dev(a, k, kc) for a in range(3) for k in NEAR for kc in range(2)] + [dev(0, 0, 1)]
    for peer in peers:
        pl.semaphore_signal(barrier, 1, device_id=peer, device_id_type=MESH)

    loads = [
        pltpu.make_async_copy(src, dst, wsem.at[i])
        for i, (src, dst) in enumerate(
            (
                (k_hbm, k_ref), (v_hbm, v_ref), (kg_hbm, kg_ref), (rtab_hbm, rtab_ref), (ctab_hbm, ctab_ref),
                (q_hbm, q_ref), (qg_hbm, qg_ref), (ids_hbm, ids_ref), (gate_hbm, gate_ref), (res_hbm, res_ref),
                (mix_hbm, mix_ref), (ffn_hbm, ffn_ref), (post_hbm, post_ref),
                (wo_hbm, wo), (wg_hbm.at[0], wg), (wu_hbm.at[0], wu), (wd_hbm.at[0], wd),
            )
        )
    ]
    for load in loads:
        load.start()

    def loaded(first_load, last_load):
        for load in loads[first_load:last_load]:
            load.wait()

    lane = lax.broadcasted_iota(jnp.int32, (TOK, 128), 1)
    even = (lane % 2) == 0
    low = lane < 64
    seg = jnp.where(
        (lax.broadcasted_iota(jnp.int32, (128, 128), 0) // 64)
        == (lax.broadcasted_iota(jnp.int32, (128, 128), 1) // 64),
        1.0 / 64.0,
        0.0,
    ).astype(BF16)
    loaded(0, 5)
    rt = rtab_ref[s]
    cos = jnp.concatenate([ctab_ref[0] + rt[0:1], ctab_ref[0] + rt[1:2]], axis=0)
    sin = jnp.concatenate([ctab_ref[1] + rt[2:3], ctab_ref[1] + rt[3:4]], axis=0)

    def turn(x, gain):
        x = x.astype(F32)
        sq = x * x
        hi = sq.astype(BF16)
        lo = (sq - hi.astype(F32)).astype(BF16)
        ms = jnp.dot(hi, seg, preferred_element_type=F32) + jnp.dot(
            lo, seg, preferred_element_type=F32
        )
        y = x * lax.rsqrt(ms + EPS) * gain
        swapped = jnp.where(even, pltpu.roll(y, 127, 1), pltpu.roll(y, 1, 1))
        return y * cos + swapped * sin

    kgain = jnp.concatenate([kg_ref[...], kg_ref[...]], axis=1)
    for p in range(2):
        cols = slice(p * 128, (p + 1) * 128)
        kv[p, 0, :, 0:128] = turn(k_ref[0, :, cols], kgain).astype(BF16)
        kv[p, 0, :, 128:256] = v_ref[0, :, cols]
        kv[p, :, :, 256:384] = jnp.ones((16, TOK, 128), BF16)

    pl.semaphore_wait(barrier, len(peers))

    def hop(p, axis, k, src, dst):
        return pltpu.make_async_remote_copy(
            src_ref=kv.at[p, src, :, pl.ds(0, 256)],
            dst_ref=kv.at[p, dst, :, pl.ds(0, 256)],
            send_sem=gs.at[p, dst // 4],
            recv_sem=gr.at[p, min(dst, 12)],
            device_id=dev(axis, k),
            device_id_type=MESH,
        )

    def gather_first(p, k1):
        return hop(p, PAIRS[p][0], k1, 0, k1)

    def gather_second(p, k2, k1):
        if k2 == 2:
            k = 1 if k1 < 2 else 3
            return hop(p, PAIRS[p][1], k, PLACE[k] * 4 + k1, PLACE[2] * 4 + k1)
        return hop(p, PAIRS[p][1], k2, k1, PLACE[k2] * 4 + k1)

    for k1 in NEAR:
        for p in range(2):
            gather_first(p, k1).start()
    for k2 in (1, 3):
        for p in range(2):
            gather_second(p, k2, 0).start()

    loaded(5, 13)
    qgain = jnp.concatenate([qg_ref[...], qg_ref[...]], axis=1)
    for b in range(8):
        t = turn(q_ref[0, :, b * 128 : (b + 1) * 128], qgain).astype(BF16).astype(F32) * 0.125
        flip = pltpu.roll(t, 64, 1)
        p, pos, i = b // 4, (b // 2) % 2, (b % 4) * 2
        if pos == 0:
            a0, a1 = jnp.where(low, t, 0.0), jnp.where(low, flip, 0.0)
        else:
            a0, a1 = jnp.where(low, 0.0, flip), jnp.where(low, 0.0, t)
        qp[p, i * 128 : (i + 1) * 128] = a0.astype(BF16)
        qp[p, (i + 1) * 128 : (i + 2) * 128] = a1.astype(BF16)

    for k1 in (1, 3, 2):
        for p in range(2):
            gather_first(p, k1).wait_recv()
            for k2 in (1, 3):
                gather_second(p, k2, k1).start()
    for p in range(2):
        gather_second(p, 1, 0).wait_recv()
        gather_second(p, 2, 0).start()

    tok_r = lax.broadcasted_iota(jnp.int32, (128, 128), 0)
    tok_c = lax.broadcasted_iota(jnp.int32, (128, 128), 1)
    before = (tok_r < tok_c).astype(F32).astype(BF16)
    idt = [ids_ref[k : k + 1, :] for k in range(2)]
    hot = [(t == tok_r).astype(F32) for t in idt]
    cnt = [jnp.dot(h.astype(BF16), before, preferred_element_type=F32) for h in hot]
    cnt[1] = cnt[1] + jnp.sum(hot[0], axis=1, keepdims=True)
    rank = [jnp.sum(h * c, axis=0, keepdims=True).astype(jnp.int32) for h, c in zip(hot, cnt)]
    slot_row = lax.broadcasted_iota(jnp.int32, (SLOTS, 128), 0)
    slot_col = lax.broadcasted_iota(jnp.int32, (128, SLOTS), 1).astype(F32)
    for p, (axes, _, _) in enumerate(PARTS):
        slots = []
        for k in range(2):
            e = idt[k]
            at = (e // 32, (e // 8) % 4, (e // 2) % 4)
            rel = [(at[a] - mine[a] + 4) % 4 for a in axes]
            kc = (e % 2 + core) % 2
            slots.append((((kc * 4 + rel[0]) * 4 + rel[1]) * 4 + rel[2]) * 4 + rank[k])
        disp[p] = ((slot_row == slots[0]) | (slot_row == slots[1])).astype(F32).astype(BF16)
        for k in range(2):
            col = jnp.transpose(jnp.broadcast_to(slots[k].astype(F32), (128, 128)))[:, 0:1]
            comb[p, k] = (slot_col == col).astype(F32).astype(BF16)

    def stripe(first_place, count, fresh):
        for p in range(2):
            span = slice(first_place * 4, (first_place + count) * 4)
            n = count * 512
            keys = kv[p, span, :, 0:128].reshape(n, 128)
            vals = kv[p, span, :, 128:384].reshape(n, 256)
            for i in range(1024 // ROWS):
                r = slice(i * ROWS, (i + 1) * ROWS)
                sc = lax.dot_general(
                    qp[p, r, :], keys, (((1,), (1,)), ((), ())), preferred_element_type=F32
                )
                top = jnp.broadcast_to(jnp.max(sc, axis=1, keepdims=True), (ROWS, 128))
                if not fresh:
                    old = mx[p, r, :]
                    top = jnp.maximum(top, old)
                    fade = jnp.exp(old - top)
                mx[p, r, :] = top
                e = jnp.exp(sc - jnp.concatenate([top] * (n // 128), axis=1)).astype(BF16)
                o = jnp.dot(e, vals, preferred_element_type=F32)
                if not fresh:
                    o = o + acc[p, r, :] * jnp.concatenate([fade, fade], axis=1)
                acc[p, r, :] = o

    stripe(0, 1, True)
    for k2, k1 in ((1, 1), (3, 3), (3, 2)):
        for p in range(2):
            gather_second(p, k2, k1).wait_recv()
            gather_second(p, 2, k1).start()
    for k2, rest in ((1, (3, 2)), (3, (0, 1))):
        for k1 in rest:
            for p in range(2):
                gather_second(p, k2, k1).wait_recv()
    stripe(1, 2, False)
    for p in range(2):
        drain(kv.at[p, pl.ds(12, 4), :, pl.ds(0, 256)], gr.at[p, 12])
    stripe(3, 1, False)

    for b in range(8):
        p, pos, i = b // 4, (b // 2) % 2, (b % 4) * 2
        o = []
        for j in (i, i + 1):
            r = slice(j * 128, (j + 1) * 128)
            o.append(acc[p, r, 0:128] / acc[p, r, 128:256])
        if pos == 0:
            a = jnp.where(low, o[0], pltpu.roll(o[1], 64, 1))
        else:
            a = jnp.where(low, pltpu.roll(o[0], 64, 1), o[1])
        att[:, b * 128 : (b + 1) * 128] = a.astype(BF16)

    loaded(13, 14)
    projected = jnp.dot(att[...], wo[...], preferred_element_type=F32)
    fr = (res_ref[0].astype(F32) + rms(projected) * mix_ref[...]).astype(BF16)
    first[...] = fr
    normed[...] = (rms(fr.astype(F32)) * ffn_ref[...]).astype(BF16)

    def cols_of(p):
        return pl.ds(PARTS[p][1], PARTS[p][2])

    def remote(src, dst, ss, rs, device):
        return pltpu.make_async_remote_copy(
            src_ref=src, dst_ref=dst, send_sem=ss, recv_sem=rs, device_id=device, device_id_type=MESH
        )

    def stage1(u, k1, back):
        w, p = u
        n = w * 3 + p
        axis = PARTS[p][0][0]
        c = cols_of(p)
        if back:
            src, dst = inboxr.at[w, k1, :, c], outr.at[w, k1, :, c]
            if k1 == 0:
                return pltpu.make_async_copy(src, dst, r3r.at[n])
            return remote(src, dst, sent.at[n, 1], r3r.at[n], dev(axis, 4 - k1))
        return remote(outbox.at[w, k1, :, c], inbox.at[w, k1, :, c], sent.at[n, 0], f1r.at[n, k1 - 1], dev(axis, k1))

    def stage2(u, k2, k1, back):
        w, p = u
        n = w * 3 + p
        axis = PARTS[p][0][1]
        c = cols_of(p)
        r = pl.ds(k2 * 16, 16)
        if back:
            return remote(midr.at[w, k2, k1, :, c], inboxr.at[w, k1, r, c], sent.at[n, 1], r2r.at[n, k1], dev(axis, 4 - k2))
        g = k1 if p == 2 else k2
        return remote(inbox.at[w, k1, r, c], mid.at[w, k2, k1, :, c], sent.at[n, 0], f2r.at[n, g], dev(axis, k2))

    def stage3(u, g, zero, k3, back):
        w, p = u
        n = w * 3 + p
        axis = PARTS[p][0][2]
        c = cols_of(p)
        r = pl.ds(k3 * 4, 4)
        box, deep, far = (inboxr, midr, ys) if back else (inbox, mid, xs)
        if p == 2:
            q = pl.ds(g * 4, 4)
            if zero:
                here, there = box.at[w, g, r, c], far.at[w, k3, 0, q, c]
            else:
                here, there = deep.at[w, pl.ds(1, 3), g, r, c], far.at[w, k3, pl.ds(1, 3), q, c]
        else:
            here = box.at[w, :, r, c] if zero else deep.at[w, g, :, r, c]
            there = far.at[w, g, :, r, c] if p == 0 else far.at[w, :, k3, pl.ds(g * 4, 4), c]
        if back:
            sem = r1z.at[n] if zero else r1r.at[n, g]
            if (k3, w) == (0, 0):
                return pltpu.make_async_copy(there, here, sem)
            return remote(there, here, sent.at[n, 1], sem, dev(axis, 4 - k3, w))
        if (k3, w) == (0, 0):
            return pltpu.make_async_copy(here, there, f3r.at[n])
        return remote(here, there, sent.at[n, 0], f3r.at[n], dev(axis, k3, w))

    def fan(u, g, zero, back):
        for k3 in NEAR + (0,):
            stage3(u, g, zero, k3, back).start()

    for u in UNITS:
        w, p = u
        c = slice(PARTS[p][1], PARTS[p][1] + PARTS[p][2])
        packed = (
            jnp.dot(disp[p, w * 256 : (w + 1) * 256], normed[:, c], preferred_element_type=F32)
            .astype(BF16)
            .reshape(4, 64, PARTS[p][2])
        )
        inbox[w, 0, :, c] = packed[0]
        outbox[w, 1:4, :, c] = packed[1:4]
        for k1 in NEAR:
            stage1(u, k1, False).start()
        for k2 in NEAR:
            stage2(u, k2, 0, False).start()
    for w in range(2):
        for k1 in (1, 3, 2):
            for p in range(3):
                u = (w, p)
                drain(inbox.at[w, k1, :, cols_of(p)], f1r.at[w * 3 + p, k1 - 1])
                for k2 in NEAR:
                    stage2(u, k2, k1, False).start()
        for p in range(3):
            u = (w, p)
            for g in range(4) if p == 2 else range(1):
                fan(u, g, True, False)
    for w in range(2):
        for i in range(4):
            for p in range(3):
                u = (w, p)
                n = w * 3 + p
                c = cols_of(p)
                if p == 2:
                    g = (0, 1, 3, 2)[i]
                    drain(mid.at[w, pl.ds(1, 3), g, :, c], f2r.at[n, g])
                    fan(u, g, False, False)
                elif i > 0:
                    g = (0, 1, 3, 2)[i]
                    drain(mid.at[w, g, :, :, c], f2r.at[n, g])
                    fan(u, g, False, False)

    for w in range(2):
        if w == 0:
            loaded(14, 17)
        for p in range(3):
            drain(xs.at[w, :, :, :, cols_of(p)], f3r.at[w * 3 + p])
        x = xs[w].reshape(256, D)
        gate = jnp.dot(x, wg[...], preferred_element_type=F32)
        up = jnp.dot(x, wu[...], preferred_element_type=F32)
        hidden = (jax.nn.silu(gate) * up).astype(BF16)
        for p in range(3):
            u = (w, p)
            c = slice(PARTS[p][1], PARTS[p][1] + PARTS[p][2])
            ys[w, :, :, :, c] = (
                jnp.dot(hidden, wd[:, c], preferred_element_type=F32)
                .astype(BF16)
                .reshape(4, 4, 16, PARTS[p][2])
            )
            for g in NEAR + (0,):
                if p == 2 or g > 0:
                    fan(u, g, False, True)
            for g in range(4) if p == 2 else range(1):
                fan(u, g, True, True)

    for w in range(2):
        for i in range(4):
            for p in range(3):
                u = (w, p)
                n = w * 3 + p
                c = cols_of(p)
                g = (NEAR + (0,))[i]
                if p == 2:
                    drain(midr.at[w, pl.ds(1, 3), g, :, c], r1r.at[n, g])
                    for k2 in NEAR:
                        stage2(u, k2, g, True).start()
                elif g > 0:
                    drain(midr.at[w, g, :, :, c], r1r.at[n, g])
                    for k1 in NEAR + (0,):
                        stage2(u, g, k1, True).start()
    for w in range(2):
        for p in range(3):
            drain(inboxr.at[w, :, pl.ds(0, 16), cols_of(p)], r1z.at[w * 3 + p])
        for k1 in NEAR + (0,):
            for p in range(3):
                drain(inboxr.at[w, k1, pl.ds(16, 48), cols_of(p)], r2r.at[w * 3 + p, k1])
                stage1((w, p), k1, True).start()

    g0, g1 = [jnp.transpose(jnp.broadcast_to(gate_ref[k : k + 1, :], (128, 128))) for k in range(2)]
    sums = [None] * 3
    for w in range(2):
        for p in range(3):
            c = slice(PARTS[p][1], PARTS[p][1] + PARTS[p][2])
            half = slice(w * 256, (w + 1) * 256)
            wide = PARTS[p][2] // 128
            drain(outr.at[w, :, :, cols_of(p)], r3r.at[w * 3 + p])
            back = outr[w, :, :, c].reshape(256, PARTS[p][2])
            a0 = jnp.dot(comb[p, 0, :, half], back, preferred_element_type=F32)
            a1 = jnp.dot(comb[p, 1, :, half], back, preferred_element_type=F32)
            term = jnp.concatenate([g0] * wide, axis=1) * a0 + jnp.concatenate([g1] * wide, axis=1) * a1
            if w == 0:
                tot[:, c] = term
            else:
                sums[p] = tot[:, c] + term
    total = jnp.concatenate(sums, axis=1)
    out_ref[0] = (first[...].astype(F32) + rms(total) * post_ref[...]).astype(BF16)

    for p in range(2):
        drain(kv.at[p, pl.ds(0, 3), :, pl.ds(0, 256)], gs.at[p, 0])
        for i in range(1, 4):
            drain(kv.at[p, pl.ds(0, 4), :, pl.ds(0, 256)], gs.at[p, i])
    for w, p in UNITS:
        n = w * 3 + p
        c = cols_of(p)
        for i in range(2):
            drain(wo.at[pl.ds(0, 576 + w * 64), c], sent.at[n, i])


def shards(
    queries, keys, values, q_gain, k_gain, residual, out_weight, mix_gain, ffn_gain, post_gain,
    expert_ids, expert_gate, w_gate, w_up, w_down,
):
    rows, cols = tables()
    vm = pl.BlockSpec(memory_space=pltpu.VMEM)
    hbm = pl.BlockSpec(memory_space=pltpu.HBM)
    sem = pltpu.SemaphoreType.DMA
    box = pltpu.VMEM((2, 4, 64, D), BF16)
    deep = pltpu.VMEM((2, 4, 4, 16, D), BF16)
    return pl.pallas_call(
        kernel,
        out_shape=jax.ShapeDtypeStruct((1, TOK, D), BF16),
        in_specs=[hbm] * 17,
        out_specs=vm,
        scratch_shapes=[
            pltpu.VMEM((1, TOK, 256), BF16), pltpu.VMEM((1, TOK, 256), BF16), pltpu.VMEM((1, 64), F32),
            pltpu.VMEM((16, 8, 128), F32), pltpu.VMEM((2, 64, 128), F32),
            pltpu.VMEM((1, TOK, 1024), BF16), pltpu.VMEM((1, 64), F32),
            pltpu.VMEM((2, TOK), jnp.int32), pltpu.VMEM((2, TOK), F32), pltpu.VMEM((1, TOK, D), BF16),
            pltpu.VMEM((1, D), F32), pltpu.VMEM((1, D), F32), pltpu.VMEM((1, D), F32),
            pltpu.VMEM((1024, D), BF16),
            pltpu.VMEM((D, 512), BF16),
            pltpu.VMEM((D, 512), BF16),
            pltpu.VMEM((512, D), BF16),
            pltpu.VMEM((2, 1024, 128), BF16),
            pltpu.VMEM((2, 16, TOK, 384), BF16),
            pltpu.VMEM((2, 1024, 128), F32),
            pltpu.VMEM((2, 1024, 256), F32),
            pltpu.VMEM((TOK, 1024), BF16),
            pltpu.VMEM((TOK, D), BF16),
            pltpu.VMEM((TOK, D), BF16),
            pltpu.VMEM((3, SLOTS, 128), BF16),
            pltpu.VMEM((3, 2, 128, SLOTS), BF16),
            box, box, deep, deep, deep, deep, box, box,
            pltpu.VMEM((TOK, D), F32),
            sem((17,)),
            sem((2, 4)), sem((2, 13)),
            sem((6, 3)), sem((6, 4)), sem((6,)),
            sem((6, 4)), sem((6,)), sem((6, 4)), sem((6,)),
            sem((6, 2)),
        ],
        compiler_params=pltpu.CompilerParams(
            collective_id=0, has_side_effects=True, vmem_limit_bytes=LIMIT
        ),
        name="layer",
    )(
        keys, values, k_gain[None], jnp.asarray(rows), jnp.asarray(cols), queries, q_gain[None],
        expert_ids[0].T, expert_gate[0].T, residual, mix_gain[None], ffn_gain[None], post_gain[None],
        out_weight, w_gate, w_up, w_down,
    )


def solution(mesh):
    return jax.shard_map(
        shards,
        mesh=mesh,
        in_specs=(
            P("dp", "sp", None), P("dp", "sp", None), P("dp", "sp", None), P(), P(),
            P("dp", "sp", None), P(), P(), P(), P(),
            P("dp", "sp", None), P("dp", "sp", None),
            P(("sp", "dp"), None, None), P(("sp", "dp"), None, None), P(("sp", "dp"), None, None),
        ),
        out_specs=P("dp", "sp", None),
        check_vma=False,
    )
```

```python
import functools

import numpy as np
import jax
import jax.numpy as jnp
from jax import lax
from jax.experimental import pallas as pl
from jax.experimental.pallas import tpu as pltpu
from jax.sharding import PartitionSpec as P

MESH = pl.DeviceIdType.MESH
F32, BF16 = jnp.float32, jnp.bfloat16
EPS = 1e-06
GRID = 64
D = 2048
TOK = 128
SLOTS = 512
ROWS = 256
LIMIT = 60 * 2**20

PARTS = (((0, 1, 2), 0, 640), ((1, 2, 0), 640, 640), ((2, 0, 1), 1280, 768))
UNITS = tuple((w, p) for w in range(2) for p in range(3))
PLACE = {
    (0, 0): 0, (0, 1): 1, (0, 2): 2, (0, 3): 3, (1, 0): 4, (3, 0): 5, (1, 1): 6, (3, 1): 7,
    (1, 3): 8, (3, 3): 9, (1, 2): 10, (3, 2): 11, (2, 0): 12, (2, 1): 13, (2, 2): 14, (2, 3): 15,
}
PAIRS = ((0, 1), (1, 0))
NEAR = (2, 1, 3)


def tables():
    lane = np.arange(128) % 64
    pair = lane // 2
    freq = 10000.0 ** (-4.0 * (pair % 16) / 64.0)
    sign = np.where(lane % 2 == 0, -1.0, 1.0)
    row_lane = pair < 16
    rows = np.zeros((16, 8, 128), np.float32)
    for s in range(16):
        for i in range(2):
            ang = (2 * s + i) * freq
            rows[s, i] = np.where(row_lane, np.cos(ang), 0.0)
            rows[s, 2 + i] = np.where(row_lane, np.sin(ang) * sign, 0.0)
    ang = np.arange(64)[:, None] * freq[None, :]
    cols = np.stack(
        [np.where(row_lane, 0.0, np.cos(ang)), np.where(row_lane, 0.0, np.sin(ang) * sign)]
    ).astype(np.float32)
    return rows, cols


def rms(v):
    return v * lax.rsqrt(jnp.mean(v * v, axis=-1, keepdims=True) + EPS)


def kernel(
    k_hbm, v_hbm, kg_hbm, rtab_hbm, ctab_hbm, q_hbm, qg_hbm, ids_hbm, gate_hbm, res_hbm,
    mix_hbm, ffn_hbm, post_hbm, wo_hbm, wg_hbm, wu_hbm, wd_hbm,
    out_ref,
    k_ref, v_ref, kg_ref, rtab_ref, ctab_ref, q_ref, qg_ref, ids_ref, gate_ref, res_ref,
    mix_ref, ffn_ref, post_ref,
    wo, wg, wu, wd, qp, kv, mx, acc, att, first, normed, disp, comb,
    ids_in, line, inbox, mid, xs, ys, midr, inboxr, outr, tot,
    wsem, idsem, gs, gr, f1s, f1r, f2r, f3r, r1r, r1z, r2r, r3r, sent,
):
    s = lax.axis_index("sp")
    d = lax.axis_index("dp")
    mine = (s // 4, s % 4, d // 2)
    core = d % 2

    def dev(axis, k, kc=0):
        p = list(mine)
        p[axis] = (p[axis] + k) % 4
        return (p[0] * 4 + p[1], p[2] * 2 + (core + kc) % 2)

    def drain(ref, sem):
        pltpu.make_async_copy(ref, ref, sem).wait()

    barrier = pltpu.get_barrier_semaphore()
    peers = [dev(a, k, kc) for a in range(3) for k in NEAR for kc in range(2)] + [dev(0, 0, 1)]
    for peer in peers:
        pl.semaphore_signal(barrier, 1, device_id=peer, device_id_type=MESH)

    loads = [
        pltpu.make_async_copy(src, dst, wsem.at[i])
        for i, (src, dst) in enumerate(
            (
                (k_hbm, k_ref), (v_hbm, v_ref), (kg_hbm, kg_ref), (rtab_hbm, rtab_ref), (ctab_hbm, ctab_ref),
                (ids_hbm, ids_ref), (q_hbm, q_ref), (qg_hbm, qg_ref), (gate_hbm, gate_ref), (res_hbm, res_ref),
                (mix_hbm, mix_ref), (ffn_hbm, ffn_ref), (post_hbm, post_ref),
                (wo_hbm, wo), (wg_hbm.at[0], wg), (wu_hbm.at[0], wu), (wd_hbm.at[0], wd),
            )
        )
    ]
    for load in loads:
        load.start()

    def loaded(first_load, last_load):
        for load in loads[first_load:last_load]:
            load.wait()

    lane = lax.broadcasted_iota(jnp.int32, (TOK, 128), 1)
    even = (lane % 2) == 0
    low = lane < 64
    seg = jnp.where(
        (lax.broadcasted_iota(jnp.int32, (128, 128), 0) // 64)
        == (lax.broadcasted_iota(jnp.int32, (128, 128), 1) // 64),
        1.0 / 64.0,
        0.0,
    ).astype(BF16)
    loaded(0, 6)
    rt = rtab_ref[s]
    cos = jnp.concatenate([ctab_ref[0] + rt[0:1], ctab_ref[0] + rt[1:2]], axis=0)
    sin = jnp.concatenate([ctab_ref[1] + rt[2:3], ctab_ref[1] + rt[3:4]], axis=0)

    def turn(x, gain):
        x = x.astype(F32)
        sq = x * x
        hi = sq.astype(BF16)
        lo = (sq - hi.astype(F32)).astype(BF16)
        ms = jnp.dot(hi, seg, preferred_element_type=F32) + jnp.dot(
            lo, seg, preferred_element_type=F32
        )
        y = x * lax.rsqrt(ms + EPS) * gain
        swapped = jnp.where(even, pltpu.roll(y, 127, 1), pltpu.roll(y, 1, 1))
        return y * cos + swapped * sin

    kgain = jnp.concatenate([kg_ref[...], kg_ref[...]], axis=1)
    for p in range(2):
        cols = slice(p * 128, (p + 1) * 128)
        kv[p, 0, :, 0:128] = turn(k_ref[0, :, cols], kgain).astype(BF16)
        kv[p, 0, :, 128:256] = v_ref[0, :, cols]
        kv[p, :, :, 256:384] = jnp.ones((16, TOK, 128), BF16)

    pl.semaphore_wait(barrier, len(peers))

    def hop(p, axis, k, src, dst):
        return pltpu.make_async_remote_copy(
            src_ref=kv.at[p, src, :, pl.ds(0, 256)],
            dst_ref=kv.at[p, dst, :, pl.ds(0, 256)],
            send_sem=gs.at[p, dst // 4],
            recv_sem=gr.at[p, min(dst, 12)],
            device_id=dev(axis, k),
            device_id_type=MESH,
        )

    def gather_first(p, k1):
        return hop(p, PAIRS[p][0], k1, 0, k1)

    def gather_second(p, k2, k1):
        if k2 == 2:
            k = 1 if k1 < 2 else 3
            return hop(p, PAIRS[p][1], k, PLACE[k, k1], PLACE[2, k1])
        return hop(p, PAIRS[p][1], k2, k1, PLACE[k2, k1])

    for k1 in NEAR:
        for p in range(2):
            gather_first(p, k1).start()
    for k2 in (1, 3):
        for p in range(2):
            gather_second(p, k2, 0).start()

    for axis in range(3):
        for k in NEAR:
            pltpu.make_async_remote_copy(
                src_ref=ids_ref,
                dst_ref=ids_in.at[axis, k],
                send_sem=idsem.at[0],
                recv_sem=idsem.at[1],
                device_id=dev(axis, k),
                device_id_type=MESH,
            ).start()

    loaded(6, 13)
    qgain = jnp.concatenate([qg_ref[...], qg_ref[...]], axis=1)
    for b in range(8):
        t = turn(q_ref[0, :, b * 128 : (b + 1) * 128], qgain).astype(BF16).astype(F32) * 0.125
        flip = pltpu.roll(t, 64, 1)
        p, pos, i = b // 4, (b // 2) % 2, (b % 4) * 2
        if pos == 0:
            a0, a1 = jnp.where(low, t, 0.0), jnp.where(low, flip, 0.0)
        else:
            a0, a1 = jnp.where(low, 0.0, flip), jnp.where(low, 0.0, t)
        qp[p, i * 128 : (i + 1) * 128] = a0.astype(BF16)
        qp[p, (i + 1) * 128 : (i + 2) * 128] = a1.astype(BF16)

    for k1 in (1, 3, 2):
        for p in range(2):
            gather_first(p, k1).wait_recv()
            for k2 in (1, 3):
                gather_second(p, k2, k1).start()
    for p in range(2):
        gather_second(p, 1, 0).wait_recv()
        gather_second(p, 2, 0).start()

    tok_r = lax.broadcasted_iota(jnp.int32, (128, 128), 0)
    tok_c = lax.broadcasted_iota(jnp.int32, (128, 128), 1)
    before = (tok_r < tok_c).astype(F32).astype(BF16)
    slot_row = lax.broadcasted_iota(jnp.int32, (128, 128), 0)
    slot_col = lax.broadcasted_iota(jnp.int32, (128, SLOTS), 1).astype(F32)

    def route(pair):
        idt = [pair[k : k + 1, :] for k in range(2)]
        hot = [(t == tok_r).astype(F32) for t in idt]
        cnt = [jnp.dot(h.astype(BF16), before, preferred_element_type=F32) for h in hot]
        cnt[1] = cnt[1] + jnp.sum(hot[0], axis=1, keepdims=True)
        rank = [jnp.sum(h * c, axis=0, keepdims=True).astype(jnp.int32) for h, c in zip(hot, cnt)]
        return list(zip(idt, rank))

    def places(e, rank, axes):
        at = (e // 32, (e // 8) % 4, (e // 2) % 4)
        rel = [(at[a] - mine[a] + 4) % 4 for a in axes]
        return rel[0], (e % 2 + core) % 2, (rel[1] * 4 + rel[2]) * 4 + rank

    def pick(p, k, routed):
        slots = []
        for e, rank in routed:
            plane, kc, r = places(e, rank, PARTS[p][0])
            slots.append(jnp.where(plane == 0, kc * 64 + r, -1))
        disp[p, k] = ((slot_row == slots[0]) | (slot_row == slots[1])).astype(F32).astype(BF16)

    own = route(ids_ref[...])
    for p, (axes, _, _) in enumerate(PARTS):
        pick(p, 0, own)
        for k, (e, rank) in enumerate(own):
            plane, kc, r = places(e, rank, axes)
            full = (kc * 4 + plane) * 64 + r
            col = jnp.transpose(jnp.broadcast_to(full.astype(F32), (128, 128)))[:, 0:1]
            comb[p, k] = (slot_col == col).astype(F32).astype(BF16)

    def stripe(first_place, count, fresh):
        for p in range(2):
            span = slice(first_place * 4, (first_place + count) * 4)
            n = count * 512
            keys = kv[p, span, :, 0:128].reshape(n, 128)
            vals = kv[p, span, :, 128:384].reshape(n, 256)
            for i in range(1024 // ROWS):
                r = slice(i * ROWS, (i + 1) * ROWS)
                sc = lax.dot_general(
                    qp[p, r, :], keys, (((1,), (1,)), ((), ())), preferred_element_type=F32
                )
                top = jnp.broadcast_to(jnp.max(sc, axis=1, keepdims=True), (ROWS, 128))
                if not fresh:
                    old = mx[p, r, :]
                    top = jnp.maximum(top, old)
                    fade = jnp.exp(old - top)
                mx[p, r, :] = top
                e = jnp.exp(sc - jnp.concatenate([top] * (n // 128), axis=1)).astype(BF16)
                o = jnp.dot(e, vals, preferred_element_type=F32)
                if not fresh:
                    o = o + acc[p, r, :] * jnp.concatenate([fade, fade], axis=1)
                acc[p, r, :] = o

    stripe(0, 1, True)

    def relay(k2, k1):
        for p in range(2):
            gather_second(p, k2, k1).wait_recv()
            gather_second(p, 2, k1).start()

    def arrive(*pieces):
        for k2, k1 in pieces:
            for p in range(2):
                gather_second(p, k2, k1).wait_recv()

    relay(1, 1)
    drain(ids_in.at[:, pl.ds(1, 3)], idsem.at[1])
    for p in range(3):
        for k in NEAR:
            pick(p, k, route(ids_in[p, k]))
    relay(3, 3)
    arrive((3, 0), (3, 1))
    stripe(1, 1, False)
    relay(3, 2)
    arrive((1, 3), (1, 2))
    stripe(2, 1, False)
    for p in range(2):
        drain(kv.at[p, pl.ds(12, 4), :, pl.ds(0, 256)], gr.at[p, 12])
    stripe(3, 1, False)

    for b in range(8):
        p, pos, i = b // 4, (b // 2) % 2, (b % 4) * 2
        o = []
        for j in (i, i + 1):
            r = slice(j * 128, (j + 1) * 128)
            o.append(acc[p, r, 0:128] / acc[p, r, 128:256])
        if pos == 0:
            a = jnp.where(low, o[0], pltpu.roll(o[1], 64, 1))
        else:
            a = jnp.where(low, pltpu.roll(o[0], 64, 1), o[1])
        att[:, b * 128 : (b + 1) * 128] = a.astype(BF16)

    loaded(13, 14)
    projected = jnp.dot(att[...], wo[...], preferred_element_type=F32)
    fr = (res_ref[0].astype(F32) + rms(projected) * mix_ref[...]).astype(BF16)
    first[...] = fr
    normed[...] = (rms(fr.astype(F32)) * ffn_ref[...]).astype(BF16)

    def cols_of(p):
        return pl.ds(PARTS[p][1], PARTS[p][2])

    def remote(src, dst, ss, rs, device):
        return pltpu.make_async_remote_copy(
            src_ref=src, dst_ref=dst, send_sem=ss, recv_sem=rs, device_id=device, device_id_type=MESH
        )

    def stage1(p, k1, relayed):
        axis = PARTS[p][0][0]
        c = cols_of(p)
        if relayed:
            r = pl.ds(0 if k1 == 1 else 64, 64)
            return remote(line.at[k1, r, c], line.at[2, r, c], f1s.at[p], f1r.at[p, 1], dev(axis, k1))
        return remote(normed.at[:, c], line.at[k1, :, c], f1s.at[p], f1r.at[p, k1 - 1], dev(axis, k1))

    def last1(u, k1):
        w, p = u
        n = w * 3 + p
        c = cols_of(p)
        src, dst = inboxr.at[w, k1, :, c], outr.at[w, k1, :, c]
        if k1 == 0:
            return pltpu.make_async_copy(src, dst, r3r.at[n])
        return remote(src, dst, sent.at[n, 1], r3r.at[n], dev(PARTS[p][0][0], 4 - k1))

    def stage2(u, k2, k1, back):
        w, p = u
        n = w * 3 + p
        axis = PARTS[p][0][1]
        c = cols_of(p)
        r = pl.ds(k2 * 16, 16)
        if back:
            return remote(midr.at[w, k2, k1, :, c], inboxr.at[w, k1, r, c], sent.at[n, 1], r2r.at[n, k1], dev(axis, 4 - k2))
        g = k1 if p == 2 else k2
        return remote(inbox.at[w, k1, r, c], mid.at[w, k2, k1, :, c], sent.at[n, 0], f2r.at[n, g], dev(axis, k2))

    def stage3(u, g, zero, k3, back):
        w, p = u
        n = w * 3 + p
        axis = PARTS[p][0][2]
        c = cols_of(p)
        r = pl.ds(k3 * 4, 4)
        box, deep, far = (inboxr, midr, ys) if back else (inbox, mid, xs)
        if p == 2:
            q = pl.ds(g * 4, 4)
            if zero:
                here, there = box.at[w, g, r, c], far.at[w, k3, 0, q, c]
            else:
                here, there = deep.at[w, pl.ds(1, 3), g, r, c], far.at[w, k3, pl.ds(1, 3), q, c]
        else:
            here = box.at[w, :, r, c] if zero else deep.at[w, g, :, r, c]
            there = far.at[w, g, :, r, c] if p == 0 else far.at[w, :, k3, pl.ds(g * 4, 4), c]
        if back:
            sem = r1z.at[n] if zero else r1r.at[n, g]
            if k3 == 0 and w == 0:
                return pltpu.make_async_copy(there, here, sem)
            return remote(there, here, sent.at[n, 1], sem, dev(axis, 4 - k3, w))
        if (k3, w) == (0, 0):
            return pltpu.make_async_copy(here, there, f3r.at[n])
        return remote(here, there, sent.at[n, 0], f3r.at[n], dev(axis, k3, w))

    def fan(u, g, zero, back):
        if not back:
            return [(k3, stage3(u, g, zero, k3, back)) for k3 in (1, 3, 0, 2)]

        @pl.when(u[0] == 0)
        def _():
            stage3((0, u[1]), g, zero, 0, back).start()

        @pl.when(u[0] == 1)
        def _():
            stage3((1, u[1]), g, zero, 0, back).start()

        return [(k3, stage3(u, g, zero, k3, back)) for k3 in (1, 3, 2)]

    def go(items):
        for far in (False, True):
            for k, copy in items:
                if (k == 2) == far:
                    copy.start()

    for k1 in (1, 3):
        for p in range(3):
            stage1(p, k1, False).start()

    def pack(p, k1):
        c = slice(PARTS[p][1], PARTS[p][1] + PARTS[p][2])
        rows = normed[:, c] if k1 == 0 else line[k1, :, c]
        packed = jnp.dot(disp[p, k1], rows, preferred_element_type=F32).astype(BF16)
        inbox[:, k1, :, c] = packed.reshape(2, 64, PARTS[p][2])
        return [(k2, stage2((w, p), k2, k1, False)) for w in range(2) for k2 in (1, 3, 2)]

    def packs(k1):
        items = []
        for p in range(3):
            items += pack(p, k1)
        go(items)

    packs(0)
    for k1 in (1, 3):
        for p in range(3):
            drain(line.at[k1, :, cols_of(p)], f1r.at[p, k1 - 1])
            stage1(p, k1, True).start()
    packs(1)
    packs(3)
    for p in range(3):
        drain(line.at[2, :, cols_of(p)], f1r.at[p, 1])
    packs(2)
    for w in range(2):
        items = []
        for p in range(3):
            for g in range(4) if p == 2 else range(1):
                items += fan((w, p), g, True, False)
        go(items)
    for w in range(2):
        for i in range(4):
            items = []
            for p in range(3):
                u = (w, p)
                n = w * 3 + p
                c = cols_of(p)
                g = (0, 1, 3, 2)[i]
                if p == 2:
                    drain(mid.at[w, pl.ds(1, 3), g, :, c], f2r.at[n, g])
                elif i > 0:
                    drain(mid.at[w, g, :, :, c], f2r.at[n, g])
                if p == 2 or i > 0:
                    items += fan(u, g, False, False)
            go(items)

    def middle():
        for w in range(2):
            for i in range(4):
                items = []
                for p in range(3):
                    u = (w, p)
                    n = w * 3 + p
                    c = cols_of(p)
                    g = (NEAR + (0,))[i]
                    if p == 2:
                        drain(midr.at[w, pl.ds(1, 3), g, :, c], r1r.at[n, g])
                        items += [(k2, stage2(u, k2, g, True)) for k2 in (1, 3, 2)]
                    elif g > 0:
                        drain(midr.at[w, g, :, :, c], r1r.at[n, g])
                        items += [(g, stage2(u, g, k1, True)) for k1 in NEAR + (0,)]
                go(items)

    for turn_no in range(2):
        w = (1 - core + turn_no) % 2
        if turn_no == 0:
            loaded(14, 17)
        for p in range(3):
            drain(xs.at[w, :, :, :, cols_of(p)], f3r.at[w * 3 + p])
        x = xs[w].reshape(256, D)
        gate = jnp.dot(x, wg[...], preferred_element_type=F32)
        up = jnp.dot(x, wu[...], preferred_element_type=F32)
        hidden = (jax.nn.silu(gate) * up).astype(BF16)
        for p in range(3):
            u = (w, p)
            c = slice(PARTS[p][1], PARTS[p][1] + PARTS[p][2])
            ys[w, :, :, :, c] = (
                jnp.dot(hidden, wd[:, c], preferred_element_type=F32)
                .astype(BF16)
                .reshape(4, 4, 16, PARTS[p][2])
            )
            items = []
            for g in NEAR + (0,):
                if p == 2 or g > 0:
                    items += fan(u, g, False, True)
            for g in range(4) if p == 2 else range(1):
                items += fan(u, g, True, True)
            go(items)
        if turn_no == 0:
            pl.when(core == 1)(middle)
        else:
            pl.when(core == 0)(middle)

    for w in range(2):
        for p in range(3):
            drain(inboxr.at[w, :, pl.ds(0, 16), cols_of(p)], r1z.at[w * 3 + p])
        for k1 in NEAR + (0,):
            for p in range(3):
                drain(inboxr.at[w, k1, pl.ds(16, 48), cols_of(p)], r2r.at[w * 3 + p, k1])
                last1((w, p), k1).start()

    g0, g1 = [jnp.transpose(jnp.broadcast_to(gate_ref[k : k + 1, :], (128, 128))) for k in range(2)]
    sums = [None] * 3
    for w in range(2):
        for p in range(3):
            c = slice(PARTS[p][1], PARTS[p][1] + PARTS[p][2])
            half = slice(w * 256, (w + 1) * 256)
            wide = PARTS[p][2] // 128
            drain(outr.at[w, :, :, cols_of(p)], r3r.at[w * 3 + p])
            back = outr[w, :, :, c].reshape(256, PARTS[p][2])
            a0 = jnp.dot(comb[p, 0, :, half], back, preferred_element_type=F32)
            a1 = jnp.dot(comb[p, 1, :, half], back, preferred_element_type=F32)
            term = jnp.concatenate([g0] * wide, axis=1) * a0 + jnp.concatenate([g1] * wide, axis=1) * a1
            if w == 0:
                tot[:, c] = term
            else:
                sums[p] = tot[:, c] + term
    total = jnp.concatenate(sums, axis=1)
    out_ref[0] = (first[...].astype(F32) + rms(total) * post_ref[...]).astype(BF16)

    for p in range(2):
        drain(kv.at[p, pl.ds(0, 3), :, pl.ds(0, 256)], gs.at[p, 0])
        for i in range(1, 4):
            drain(kv.at[p, pl.ds(0, 4), :, pl.ds(0, 256)], gs.at[p, i])
    drain(ids_in.at[:, pl.ds(1, 3)], idsem.at[0])
    for p in range(3):
        drain(wo.at[pl.ds(0, 384), cols_of(p)], f1s.at[p])
    for w, p in UNITS:
        n = w * 3 + p
        c = cols_of(p)
        drain(wo.at[pl.ds(0, 384 + w * 64), c], sent.at[n, 0])
        drain(wo.at[pl.ds(0, 576 + w * 64), c], sent.at[n, 1])


def shards(
    queries, keys, values, q_gain, k_gain, residual, out_weight, mix_gain, ffn_gain, post_gain,
    expert_ids, expert_gate, w_gate, w_up, w_down,
):
    rows, cols = tables()
    vm = pl.BlockSpec(memory_space=pltpu.VMEM)
    hbm = pl.BlockSpec(memory_space=pltpu.HBM)
    sem = pltpu.SemaphoreType.DMA
    box = pltpu.VMEM((2, 4, 64, D), BF16)
    deep = pltpu.VMEM((2, 4, 4, 16, D), BF16)
    return pl.pallas_call(
        kernel,
        out_shape=jax.ShapeDtypeStruct((1, TOK, D), BF16),
        in_specs=[hbm] * 17,
        out_specs=vm,
        scratch_shapes=[
            pltpu.VMEM((1, TOK, 256), BF16), pltpu.VMEM((1, TOK, 256), BF16), pltpu.VMEM((1, 64), F32),
            pltpu.VMEM((16, 8, 128), F32), pltpu.VMEM((2, 64, 128), F32),
            pltpu.VMEM((1, TOK, 1024), BF16), pltpu.VMEM((1, 64), F32),
            pltpu.VMEM((2, TOK), jnp.int32), pltpu.VMEM((2, TOK), F32), pltpu.VMEM((1, TOK, D), BF16),
            pltpu.VMEM((1, D), F32), pltpu.VMEM((1, D), F32), pltpu.VMEM((1, D), F32),
            pltpu.VMEM((1024, D), BF16),
            pltpu.VMEM((D, 512), BF16),
            pltpu.VMEM((D, 512), BF16),
            pltpu.VMEM((512, D), BF16),
            pltpu.VMEM((2, 1024, 128), BF16),
            pltpu.VMEM((2, 16, TOK, 384), BF16),
            pltpu.VMEM((2, 1024, 128), F32),
            pltpu.VMEM((2, 1024, 256), F32),
            pltpu.VMEM((TOK, 1024), BF16),
            pltpu.VMEM((TOK, D), BF16),
            pltpu.VMEM((TOK, D), BF16),
            pltpu.VMEM((3, 4, 128, 128), BF16),
            pltpu.VMEM((3, 2, 128, SLOTS), BF16),
            pltpu.VMEM((3, 4, 2, TOK), jnp.int32),
            pltpu.VMEM((4, TOK, D), BF16),
            box, deep, deep, deep, deep, box, box,
            pltpu.VMEM((TOK, D), F32),
            sem((17,)), sem((2,)),
            sem((2, 4)), sem((2, 13)),
            sem((3,)), sem((3, 3)), sem((6, 4)), sem((6,)),
            sem((6, 4)), sem((6,)), sem((6, 4)), sem((6,)),
            sem((6, 2)),
        ],
        compiler_params=pltpu.CompilerParams(
            collective_id=0, has_side_effects=True, vmem_limit_bytes=LIMIT
        ),
        name="layer",
    )(
        keys, values, k_gain[None], jnp.asarray(rows), jnp.asarray(cols), queries, q_gain[None],
        expert_ids[0].T, expert_gate[0].T, residual, mix_gain[None], ffn_gain[None], post_gain[None],
        out_weight, w_gate, w_up, w_down,
    )


def solution(mesh):
    return jax.shard_map(
        shards,
        mesh=mesh,
        in_specs=(
            P("dp", "sp", None), P("dp", "sp", None), P("dp", "sp", None), P(), P(),
            P("dp", "sp", None), P(), P(), P(), P(),
            P("dp", "sp", None), P("dp", "sp", None),
            P(("sp", "dp"), None, None), P(("sp", "dp"), None, None), P(("sp", "dp"), None, None),
        ),
        out_specs=P("dp", "sp", None),
        check_vma=False,
    )
```

```python
import functools

import numpy as np
import jax
import jax.numpy as jnp
from jax import lax
from jax.experimental import pallas as pl
from jax.experimental.pallas import tpu as pltpu
from jax.sharding import PartitionSpec as P

MESH = pl.DeviceIdType.MESH
F32, BF16 = jnp.float32, jnp.bfloat16
EPS = 1e-06
GRID = 64
D = 2048
TOK = 128
SLOTS = 512
ROWS = 256
LIMIT = 60 * 2**20

PARTS = (((0, 1, 2), 0, 640), ((1, 2, 0), 640, 640), ((2, 0, 1), 1280, 768))
UNITS = tuple((w, p) for w in range(2) for p in range(3))
PLACE = {
    (0, 0): 0, (0, 1): 1, (0, 2): 2, (0, 3): 3, (1, 0): 4, (3, 0): 5, (1, 1): 6, (3, 1): 7,
    (1, 3): 8, (3, 3): 9, (1, 2): 10, (3, 2): 11, (2, 0): 12, (2, 1): 13, (2, 2): 14, (2, 3): 15,
}
PAIRS = ((0, 1), (1, 0))
NEAR = (2, 1, 3)


def tables():
    lane = np.arange(128) % 64
    pair = lane // 2
    freq = 10000.0 ** (-4.0 * (pair % 16) / 64.0)
    sign = np.where(lane % 2 == 0, -1.0, 1.0)
    row_lane = pair < 16
    rows = np.zeros((16, 8, 128), np.float32)
    for s in range(16):
        for i in range(2):
            ang = (2 * s + i) * freq
            rows[s, i] = np.where(row_lane, np.cos(ang), 0.0)
            rows[s, 2 + i] = np.where(row_lane, np.sin(ang) * sign, 0.0)
    ang = np.arange(64)[:, None] * freq[None, :]
    cols = np.stack(
        [np.where(row_lane, 0.0, np.cos(ang)), np.where(row_lane, 0.0, np.sin(ang) * sign)]
    ).astype(np.float32)
    return rows, cols


def rms(v):
    return v * lax.rsqrt(jnp.mean(v * v, axis=-1, keepdims=True) + EPS)


def kernel(
    k_hbm, v_hbm, kg_hbm, rtab_hbm, ctab_hbm, q_hbm, qg_hbm, ids_hbm, gate_hbm, res_hbm,
    mix_hbm, ffn_hbm, post_hbm, wo_hbm, wg_hbm, wu_hbm, wd_hbm,
    out_ref,
    k_ref, v_ref, kg_ref, rtab_ref, ctab_ref, q_ref, qg_ref, ids_ref, gate_ref, res_ref,
    mix_ref, ffn_ref, post_ref,
    wo, wg, wu, wd, qp, kv, mx, acc, att, first, normed, disp, comb,
    ids_in, line, inbox, mid, xs, ys, midr, inboxr, outr, tot,
    wsem, idsem, gs, gr, f1s, f1r, f2r, f3r, r1r, r1z, r2r, r3r, sent,
):
    s = lax.axis_index("sp")
    d = lax.axis_index("dp")
    mine = (s // 4, s % 4, d // 2)
    core = d % 2

    def dev(axis, k, kc=0):
        p = list(mine)
        p[axis] = (p[axis] + k) % 4
        return (p[0] * 4 + p[1], p[2] * 2 + (core + kc) % 2)

    def drain(ref, sem):
        pltpu.make_async_copy(ref, ref, sem).wait()

    barrier = pltpu.get_barrier_semaphore()
    peers = [dev(a, k, kc) for a in range(3) for k in NEAR for kc in range(2)] + [dev(0, 0, 1)]
    for peer in peers:
        pl.semaphore_signal(barrier, 1, device_id=peer, device_id_type=MESH)

    loads = [
        pltpu.make_async_copy(src, dst, wsem.at[i])
        for i, (src, dst) in enumerate(
            (
                (k_hbm, k_ref), (v_hbm, v_ref), (kg_hbm, kg_ref), (rtab_hbm, rtab_ref), (ctab_hbm, ctab_ref),
                (ids_hbm, ids_ref), (q_hbm, q_ref), (qg_hbm, qg_ref), (gate_hbm, gate_ref), (res_hbm, res_ref),
                (mix_hbm, mix_ref), (ffn_hbm, ffn_ref), (post_hbm, post_ref),
                (wo_hbm, wo), (wg_hbm.at[0], wg), (wu_hbm.at[0], wu), (wd_hbm.at[0], wd),
            )
        )
    ]
    for load in loads:
        load.start()

    def loaded(first_load, last_load):
        for load in loads[first_load:last_load]:
            load.wait()

    lane = lax.broadcasted_iota(jnp.int32, (TOK, 128), 1)
    even = (lane % 2) == 0
    low = lane < 64
    seg = jnp.where(
        (lax.broadcasted_iota(jnp.int32, (128, 128), 0) // 64)
        == (lax.broadcasted_iota(jnp.int32, (128, 128), 1) // 64),
        1.0 / 64.0,
        0.0,
    ).astype(BF16)
    loaded(0, 6)
    rt = rtab_ref[s]
    cos = jnp.concatenate([ctab_ref[0] + rt[0:1], ctab_ref[0] + rt[1:2]], axis=0)
    sin = jnp.concatenate([ctab_ref[1] + rt[2:3], ctab_ref[1] + rt[3:4]], axis=0)

    def turn(x, gain):
        x = x.astype(F32)
        sq = x * x
        hi = sq.astype(BF16)
        lo = (sq - hi.astype(F32)).astype(BF16)
        ms = jnp.dot(hi, seg, preferred_element_type=F32) + jnp.dot(
            lo, seg, preferred_element_type=F32
        )
        y = x * lax.rsqrt(ms + EPS) * gain
        swapped = jnp.where(even, pltpu.roll(y, 127, 1), pltpu.roll(y, 1, 1))
        return y * cos + swapped * sin

    kgain = jnp.concatenate([kg_ref[...], kg_ref[...]], axis=1)
    for p in range(2):
        cols = slice(p * 128, (p + 1) * 128)
        kv[p, 0, :, 0:128] = turn(k_ref[0, :, cols], kgain).astype(BF16)
        kv[p, 0, :, 128:256] = v_ref[0, :, cols]
        kv[p, :, :, 256:384] = jnp.ones((16, TOK, 128), BF16)

    pl.semaphore_wait(barrier, len(peers))

    def hop(p, axis, k, src, dst):
        return pltpu.make_async_remote_copy(
            src_ref=kv.at[p, src, :, pl.ds(0, 256)],
            dst_ref=kv.at[p, dst, :, pl.ds(0, 256)],
            send_sem=gs.at[p, dst // 4],
            recv_sem=gr.at[p, min(dst, 12)],
            device_id=dev(axis, k),
            device_id_type=MESH,
        )

    def gather_first(p, k1):
        return hop(p, PAIRS[p][0], k1, 0, k1)

    def gather_second(p, k2, k1):
        if k2 == 2:
            k = 1 if k1 < 2 else 3
            return hop(p, PAIRS[p][1], k, PLACE[k, k1], PLACE[2, k1])
        return hop(p, PAIRS[p][1], k2, k1, PLACE[k2, k1])

    for k1 in NEAR:
        for p in range(2):
            gather_first(p, k1).start()
    for k2 in (1, 3):
        for p in range(2):
            gather_second(p, k2, 0).start()

    for axis in range(3):
        for k in NEAR:
            pltpu.make_async_remote_copy(
                src_ref=ids_ref,
                dst_ref=ids_in.at[axis, k],
                send_sem=idsem.at[0],
                recv_sem=idsem.at[1],
                device_id=dev(axis, k),
                device_id_type=MESH,
            ).start()

    loaded(6, 13)
    qgain = jnp.concatenate([qg_ref[...], qg_ref[...]], axis=1)
    for b in range(8):
        t = turn(q_ref[0, :, b * 128 : (b + 1) * 128], qgain).astype(BF16).astype(F32) * 0.125
        flip = pltpu.roll(t, 64, 1)
        p, pos, i = b // 4, (b // 2) % 2, (b % 4) * 2
        if pos == 0:
            a0, a1 = jnp.where(low, t, 0.0), jnp.where(low, flip, 0.0)
        else:
            a0, a1 = jnp.where(low, 0.0, flip), jnp.where(low, 0.0, t)
        qp[p, i * 128 : (i + 1) * 128] = a0.astype(BF16)
        qp[p, (i + 1) * 128 : (i + 2) * 128] = a1.astype(BF16)

    for k1 in (1, 3, 2):
        for p in range(2):
            gather_first(p, k1).wait_recv()
            for k2 in (1, 3):
                gather_second(p, k2, k1).start()
    for p in range(2):
        gather_second(p, 1, 0).wait_recv()
        gather_second(p, 2, 0).start()

    tok_r = lax.broadcasted_iota(jnp.int32, (128, 128), 0)
    tok_c = lax.broadcasted_iota(jnp.int32, (128, 128), 1)
    before = (tok_r < tok_c).astype(F32).astype(BF16)
    slot_row = lax.broadcasted_iota(jnp.int32, (128, 128), 0)
    slot_col = lax.broadcasted_iota(jnp.int32, (128, SLOTS), 1).astype(F32)

    def route(pair):
        idt = [pair[k : k + 1, :] for k in range(2)]
        hot = [(t == tok_r).astype(F32) for t in idt]
        cnt = [jnp.dot(h.astype(BF16), before, preferred_element_type=F32) for h in hot]
        cnt[1] = cnt[1] + jnp.sum(hot[0], axis=1, keepdims=True)
        rank = [jnp.sum(h * c, axis=0, keepdims=True).astype(jnp.int32) for h, c in zip(hot, cnt)]
        return list(zip(idt, rank))

    def places(e, rank, axes):
        at = (e // 32, (e // 8) % 4, (e // 2) % 4)
        rel = [(at[a] - mine[a] + 4) % 4 for a in axes]
        return rel[0], (e % 2 + core) % 2, (rel[1] * 4 + rel[2]) * 4 + rank

    def pick(p, k, routed):
        slots = []
        for e, rank in routed:
            plane, kc, r = places(e, rank, PARTS[p][0])
            slots.append(jnp.where(plane == 0, kc * 64 + r, -1))
        disp[p, k] = ((slot_row == slots[0]) | (slot_row == slots[1])).astype(F32).astype(BF16)

    own = route(ids_ref[...])
    for p, (axes, _, _) in enumerate(PARTS):
        pick(p, 0, own)
        for k, (e, rank) in enumerate(own):
            plane, kc, r = places(e, rank, axes)
            full = (kc * 4 + plane) * 64 + r
            col = jnp.transpose(jnp.broadcast_to(full.astype(F32), (128, 128)))[:, 0:1]
            comb[p, k] = (slot_col == col).astype(F32).astype(BF16)

    def stripe(first_place, count, fresh):
        for p in range(2):
            span = slice(first_place * 4, (first_place + count) * 4)
            n = count * 512
            keys = kv[p, span, :, 0:128].reshape(n, 128)
            vals = kv[p, span, :, 128:384].reshape(n, 256)
            for i in range(1024 // ROWS):
                r = slice(i * ROWS, (i + 1) * ROWS)
                sc = lax.dot_general(
                    qp[p, r, :], keys, (((1,), (1,)), ((), ())), preferred_element_type=F32
                )
                top = jnp.broadcast_to(jnp.max(sc, axis=1, keepdims=True), (ROWS, 128))
                if not fresh:
                    old = mx[p, r, :]
                    top = jnp.maximum(top, old)
                    fade = jnp.exp(old - top)
                mx[p, r, :] = top
                e = jnp.exp(sc - jnp.concatenate([top] * (n // 128), axis=1)).astype(BF16)
                o = jnp.dot(e, vals, preferred_element_type=F32)
                if not fresh:
                    o = o + acc[p, r, :] * jnp.concatenate([fade, fade], axis=1)
                acc[p, r, :] = o

    stripe(0, 1, True)

    def relay(k2, k1):
        for p in range(2):
            gather_second(p, k2, k1).wait_recv()
            gather_second(p, 2, k1).start()

    def arrive(*pieces):
        for k2, k1 in pieces:
            for p in range(2):
                gather_second(p, k2, k1).wait_recv()

    relay(1, 1)
    drain(ids_in.at[:, pl.ds(1, 3)], idsem.at[1])
    for p in range(3):
        for k in NEAR:
            pick(p, k, route(ids_in[p, k]))
    relay(3, 3)
    arrive((3, 0), (3, 1))
    stripe(1, 1, False)
    relay(3, 2)
    arrive((1, 3), (1, 2))
    stripe(2, 1, False)
    for p in range(2):
        drain(kv.at[p, pl.ds(12, 4), :, pl.ds(0, 256)], gr.at[p, 12])
    stripe(3, 1, False)

    for b in range(8):
        p, pos, i = b // 4, (b // 2) % 2, (b % 4) * 2
        o = []
        for j in (i, i + 1):
            r = slice(j * 128, (j + 1) * 128)
            o.append(acc[p, r, 0:128] / acc[p, r, 128:256])
        if pos == 0:
            a = jnp.where(low, o[0], pltpu.roll(o[1], 64, 1))
        else:
            a = jnp.where(low, pltpu.roll(o[0], 64, 1), o[1])
        att[:, b * 128 : (b + 1) * 128] = a.astype(BF16)

    loaded(13, 14)
    projected = jnp.dot(att[...], wo[...], preferred_element_type=F32)
    fr = (res_ref[0].astype(F32) + rms(projected) * mix_ref[...]).astype(BF16)
    first[...] = fr
    normed[...] = (rms(fr.astype(F32)) * ffn_ref[...]).astype(BF16)

    def cols_of(p):
        return pl.ds(PARTS[p][1], PARTS[p][2])

    def remote(src, dst, ss, rs, device):
        return pltpu.make_async_remote_copy(
            src_ref=src, dst_ref=dst, send_sem=ss, recv_sem=rs, device_id=device, device_id_type=MESH
        )

    def stage1(p, k1, relayed):
        axis = PARTS[p][0][0]
        c = cols_of(p)
        if relayed:
            r = pl.ds(0 if k1 == 1 else 64, 64)
            return remote(line.at[k1, r, c], line.at[2, r, c], f1s.at[p], f1r.at[p, 1], dev(axis, k1))
        return remote(normed.at[:, c], line.at[k1, :, c], f1s.at[p], f1r.at[p, k1 - 1], dev(axis, k1))

    def last1(u, k1):
        w, p = u
        n = w * 3 + p
        c = cols_of(p)
        src, dst = inboxr.at[w, k1, :, c], outr.at[w, k1, :, c]
        if k1 == 0:
            return pltpu.make_async_copy(src, dst, r3r.at[n])
        return remote(src, dst, sent.at[n, 1], r3r.at[n], dev(PARTS[p][0][0], 4 - k1))

    def stage2(u, k2, k1, back):
        w, p = u
        n = w * 3 + p
        axis = PARTS[p][0][1]
        c = cols_of(p)
        r = pl.ds(k2 * 16, 16)
        if back:
            return remote(midr.at[w, k2, k1, :, c], inboxr.at[w, k1, r, c], sent.at[n, 1], r2r.at[n, k1], dev(axis, 4 - k2))
        g = k1 if p == 2 else k2
        return remote(inbox.at[w, k1, r, c], mid.at[w, k2, k1, :, c], sent.at[n, 0], f2r.at[n, g], dev(axis, k2))

    def stage3(u, g, zero, k3, back):
        w, p = u
        n = w * 3 + p
        axis = PARTS[p][0][2]
        c = cols_of(p)
        r = pl.ds(k3 * 4, 4)
        box, deep, far = (inboxr, midr, ys) if back else (inbox, mid, xs)
        if p == 2:
            q = pl.ds(g * 4, 4)
            if zero:
                here, there = box.at[w, g, r, c], far.at[w, k3, 0, q, c]
            else:
                here, there = deep.at[w, pl.ds(1, 3), g, r, c], far.at[w, k3, pl.ds(1, 3), q, c]
        else:
            here = box.at[w, :, r, c] if zero else deep.at[w, g, :, r, c]
            there = far.at[w, g, :, r, c] if p == 0 else far.at[w, :, k3, pl.ds(g * 4, 4), c]
        if back:
            sem = r1z.at[n] if zero else r1r.at[n, g]
            if k3 == 0 and w == 0:
                return pltpu.make_async_copy(there, here, sem)
            return remote(there, here, sent.at[n, 1], sem, dev(axis, 4 - k3, w))
        if (k3, w) == (0, 0):
            return pltpu.make_async_copy(here, there, f3r.at[n])
        return remote(here, there, sent.at[n, 0], f3r.at[n], dev(axis, k3, w))

    def fan(u, g, zero, back):
        if not back:
            return [(k3, stage3(u, g, zero, k3, back)) for k3 in (1, 3, 0, 2)]

        @pl.when(u[0] == 0)
        def _():
            stage3((0, u[1]), g, zero, 0, back).start()

        @pl.when(u[0] == 1)
        def _():
            stage3((1, u[1]), g, zero, 0, back).start()

        return [(k3, stage3(u, g, zero, k3, back)) for k3 in (1, 3, 2)]

    def go(items):
        for far in (False, True):
            for k, copy in items:
                if (k == 2) == far:
                    copy.start()

    for k1 in (1, 3):
        for p in range(3):
            stage1(p, k1, False).start()

    def pack(p, k1):
        c = slice(PARTS[p][1], PARTS[p][1] + PARTS[p][2])
        rows = normed[:, c] if k1 == 0 else line[k1, :, c]
        packed = jnp.dot(disp[p, k1], rows, preferred_element_type=F32).astype(BF16)
        inbox[:, k1, :, c] = packed.reshape(2, 64, PARTS[p][2])
        return [(k2, stage2((w, p), k2, k1, False)) for w in range(2) for k2 in (1, 3, 2)]

    def packs(k1):
        items = []
        for p in range(3):
            items += pack(p, k1)
        go(items)

    packs(0)
    for k1 in (1, 3):
        for p in range(3):
            drain(line.at[k1, :, cols_of(p)], f1r.at[p, k1 - 1])
            stage1(p, k1, True).start()
    packs(1)
    packs(3)
    for p in range(3):
        drain(line.at[2, :, cols_of(p)], f1r.at[p, 1])
    packs(2)
    for w in range(2):
        items = []
        for p in range(3):
            for g in range(4) if p == 2 else range(1):
                items += fan((w, p), g, True, False)
        go(items)
    for w in range(2):
        for i in range(4):
            items = []
            for p in range(3):
                u = (w, p)
                n = w * 3 + p
                c = cols_of(p)
                g = (0, 1, 3, 2)[i]
                if p == 2:
                    drain(mid.at[w, pl.ds(1, 3), g, :, c], f2r.at[n, g])
                elif i > 0:
                    drain(mid.at[w, g, :, :, c], f2r.at[n, g])
                if p == 2 or i > 0:
                    items += fan(u, g, False, False)
            go(items)

    def middle(waves):
        for w in waves:
            for i in range(4):
                items = []
                for p in range(3):
                    u = (w, p)
                    n = w * 3 + p
                    c = cols_of(p)
                    g = (NEAR + (0,))[i]
                    if p == 2:
                        drain(midr.at[w, pl.ds(1, 3), g, :, c], r1r.at[n, g])
                        items += [(k2, stage2(u, k2, g, True)) for k2 in (1, 3, 2)]
                    elif g > 0:
                        drain(midr.at[w, g, :, :, c], r1r.at[n, g])
                        items += [(g, stage2(u, g, k1, True)) for k1 in NEAR + (0,)]
                go(items)

    for turn_no in range(2):
        w = (1 - core + turn_no) % 2
        if turn_no == 0:
            loaded(14, 17)
        for p in range(3):
            drain(xs.at[w, :, :, :, cols_of(p)], f3r.at[w * 3 + p])
        x = xs[w].reshape(256, D)
        gate = jnp.dot(x, wg[...], preferred_element_type=F32)
        up = jnp.dot(x, wu[...], preferred_element_type=F32)
        hidden = (jax.nn.silu(gate) * up).astype(BF16)
        for p in range(3):
            u = (w, p)
            c = slice(PARTS[p][1], PARTS[p][1] + PARTS[p][2])
            ys[w, :, :, :, c] = (
                jnp.dot(hidden, wd[:, c], preferred_element_type=F32)
                .astype(BF16)
                .reshape(4, 4, 16, PARTS[p][2])
            )
            items = []
            for g in NEAR + (0,):
                if p == 2 or g > 0:
                    items += fan(u, g, False, True)
            for g in range(4) if p == 2 else range(1):
                items += fan(u, g, True, True)
            go(items)
        if turn_no == 0:
            pl.when(core == 1)(lambda: middle((0,)))
        else:
            pl.when(core == 1)(lambda: middle((1,)))
            pl.when(core == 0)(lambda: middle((0, 1)))

    for w in range(2):
        for p in range(3):
            drain(inboxr.at[w, :, pl.ds(0, 16), cols_of(p)], r1z.at[w * 3 + p])
        for k1 in NEAR + (0,):
            for p in range(3):
                drain(inboxr.at[w, k1, pl.ds(16, 48), cols_of(p)], r2r.at[w * 3 + p, k1])
                last1((w, p), k1).start()

    g0, g1 = [jnp.transpose(jnp.broadcast_to(gate_ref[k : k + 1, :], (128, 128))) for k in range(2)]
    sums = [None] * 3
    for w in range(2):
        for p in range(3):
            c = slice(PARTS[p][1], PARTS[p][1] + PARTS[p][2])
            half = slice(w * 256, (w + 1) * 256)
            wide = PARTS[p][2] // 128
            drain(outr.at[w, :, :, cols_of(p)], r3r.at[w * 3 + p])
            back = outr[w, :, :, c].reshape(256, PARTS[p][2])
            a0 = jnp.dot(comb[p, 0, :, half], back, preferred_element_type=F32)
            a1 = jnp.dot(comb[p, 1, :, half], back, preferred_element_type=F32)
            term = jnp.concatenate([g0] * wide, axis=1) * a0 + jnp.concatenate([g1] * wide, axis=1) * a1
            if w == 0:
                tot[:, c] = term
            else:
                sums[p] = tot[:, c] + term
    total = jnp.concatenate(sums, axis=1)
    out_ref[0] = (first[...].astype(F32) + rms(total) * post_ref[...]).astype(BF16)

    for p in range(2):
        drain(kv.at[p, pl.ds(0, 3), :, pl.ds(0, 256)], gs.at[p, 0])
        for i in range(1, 4):
            drain(kv.at[p, pl.ds(0, 4), :, pl.ds(0, 256)], gs.at[p, i])
    drain(ids_in.at[:, pl.ds(1, 3)], idsem.at[0])
    for p in range(3):
        drain(wo.at[pl.ds(0, 384), cols_of(p)], f1s.at[p])
    for w, p in UNITS:
        n = w * 3 + p
        c = cols_of(p)
        drain(wo.at[pl.ds(0, 384 + w * 64), c], sent.at[n, 0])
        drain(wo.at[pl.ds(0, 576 + w * 64), c], sent.at[n, 1])


def shards(
    queries, keys, values, q_gain, k_gain, residual, out_weight, mix_gain, ffn_gain, post_gain,
    expert_ids, expert_gate, w_gate, w_up, w_down,
):
    rows, cols = tables()
    vm = pl.BlockSpec(memory_space=pltpu.VMEM)
    hbm = pl.BlockSpec(memory_space=pltpu.HBM)
    sem = pltpu.SemaphoreType.DMA
    box = pltpu.VMEM((2, 4, 64, D), BF16)
    deep = pltpu.VMEM((2, 4, 4, 16, D), BF16)
    return pl.pallas_call(
        kernel,
        out_shape=jax.ShapeDtypeStruct((1, TOK, D), BF16),
        in_specs=[hbm] * 17,
        out_specs=vm,
        scratch_shapes=[
            pltpu.VMEM((1, TOK, 256), BF16), pltpu.VMEM((1, TOK, 256), BF16), pltpu.VMEM((1, 64), F32),
            pltpu.VMEM((16, 8, 128), F32), pltpu.VMEM((2, 64, 128), F32),
            pltpu.VMEM((1, TOK, 1024), BF16), pltpu.VMEM((1, 64), F32),
            pltpu.VMEM((2, TOK), jnp.int32), pltpu.VMEM((2, TOK), F32), pltpu.VMEM((1, TOK, D), BF16),
            pltpu.VMEM((1, D), F32), pltpu.VMEM((1, D), F32), pltpu.VMEM((1, D), F32),
            pltpu.VMEM((1024, D), BF16),
            pltpu.VMEM((D, 512), BF16),
            pltpu.VMEM((D, 512), BF16),
            pltpu.VMEM((512, D), BF16),
            pltpu.VMEM((2, 1024, 128), BF16),
            pltpu.VMEM((2, 16, TOK, 384), BF16),
            pltpu.VMEM((2, 1024, 128), F32),
            pltpu.VMEM((2, 1024, 256), F32),
            pltpu.VMEM((TOK, 1024), BF16),
            pltpu.VMEM((TOK, D), BF16),
            pltpu.VMEM((TOK, D), BF16),
            pltpu.VMEM((3, 4, 128, 128), BF16),
            pltpu.VMEM((3, 2, 128, SLOTS), BF16),
            pltpu.VMEM((3, 4, 2, TOK), jnp.int32),
            pltpu.VMEM((4, TOK, D), BF16),
            box, deep, deep, deep, deep, box, box,
            pltpu.VMEM((TOK, D), F32),
            sem((17,)), sem((2,)),
            sem((2, 4)), sem((2, 13)),
            sem((3,)), sem((3, 3)), sem((6, 4)), sem((6,)),
            sem((6, 4)), sem((6,)), sem((6, 4)), sem((6,)),
            sem((6, 2)),
        ],
        compiler_params=pltpu.CompilerParams(
            collective_id=0, has_side_effects=True, vmem_limit_bytes=LIMIT
        ),
        name="layer",
    )(
        keys, values, k_gain[None], jnp.asarray(rows), jnp.asarray(cols), queries, q_gain[None],
        expert_ids[0].T, expert_gate[0].T, residual, mix_gain[None], ffn_gain[None], post_gain[None],
        out_weight, w_gate, w_up, w_down,
    )


def solution(mesh):
    return jax.shard_map(
        shards,
        mesh=mesh,
        in_specs=(
            P("dp", "sp", None), P("dp", "sp", None), P("dp", "sp", None), P(), P(),
            P("dp", "sp", None), P(), P(), P(), P(),
            P("dp", "sp", None), P("dp", "sp", None),
            P(("sp", "dp"), None, None), P(("sp", "dp"), None, None), P(("sp", "dp"), None, None),
        ),
        out_specs=P("dp", "sp", None),
        check_vma=False,
    )
```

```python
import functools

import numpy as np
import jax
import jax.numpy as jnp
from jax import lax
from jax.experimental import pallas as pl
from jax.experimental.pallas import tpu as pltpu
from jax.sharding import PartitionSpec as P

MESH = pl.DeviceIdType.MESH
F32, BF16 = jnp.float32, jnp.bfloat16
EPS = 1e-06
GRID = 64
D = 2048
TOK = 128
SLOTS = 512
ROWS = 256
LIMIT = 60 * 2**20

PARTS = (((0, 1, 2), 0, 640), ((1, 2, 0), 640, 640), ((2, 0, 1), 1280, 768))
UNITS = tuple((w, p) for w in range(2) for p in range(3))
PLACE = {
    (0, 0): 0, (0, 1): 1, (0, 2): 2, (0, 3): 3, (1, 0): 4, (3, 0): 5, (1, 1): 6, (3, 1): 7,
    (1, 3): 8, (3, 3): 9, (1, 2): 10, (3, 2): 11, (2, 0): 12, (2, 1): 13, (2, 2): 14, (2, 3): 15,
}
PAIRS = ((0, 1), (1, 0))
NEAR = (2, 1, 3)


def tables():
    lane = np.arange(128) % 64
    pair = lane // 2
    freq = 10000.0 ** (-4.0 * (pair % 16) / 64.0)
    sign = np.where(lane % 2 == 0, -1.0, 1.0)
    row_lane = pair < 16
    rows = np.zeros((16, 8, 128), np.float32)
    for s in range(16):
        for i in range(2):
            ang = (2 * s + i) * freq
            rows[s, i] = np.where(row_lane, np.cos(ang), 0.0)
            rows[s, 2 + i] = np.where(row_lane, np.sin(ang) * sign, 0.0)
    ang = np.arange(64)[:, None] * freq[None, :]
    cols = np.stack(
        [np.where(row_lane, 0.0, np.cos(ang)), np.where(row_lane, 0.0, np.sin(ang) * sign)]
    ).astype(np.float32)
    return rows, cols


def rms(v):
    return v * lax.rsqrt(jnp.mean(v * v, axis=-1, keepdims=True) + EPS)


def kernel(
    k_hbm, v_hbm, kg_hbm, rtab_hbm, ctab_hbm, q_hbm, qg_hbm, ids_hbm, gate_hbm, res_hbm,
    mix_hbm, ffn_hbm, post_hbm, wo_hbm, wg_hbm, wu_hbm, wd_hbm,
    out_ref,
    k_ref, v_ref, kg_ref, rtab_ref, ctab_ref, q_ref, qg_ref, ids_ref, gate_ref, res_ref,
    mix_ref, ffn_ref, post_ref,
    wo, wg, wu, wd, qp, kv, mx, acc, att, first, normed, disp, comb,
    ids_in, line, inbox, mid, xs, ys, midr, inboxr, outr, tot,
    wsem, idsem, gs, gr, f1s, f1r, f2r, f3r, r1r, r1z, r2r, r3r, sent,
):
    s = lax.axis_index("sp")
    d = lax.axis_index("dp")
    mine = (s // 4, s % 4, d // 2)
    core = d % 2

    def dev(axis, k, kc=0):
        p = list(mine)
        p[axis] = (p[axis] + k) % 4
        return (p[0] * 4 + p[1], p[2] * 2 + (core + kc) % 2)

    def drain(ref, sem):
        pltpu.make_async_copy(ref, ref, sem).wait()

    barrier = pltpu.get_barrier_semaphore()
    peers = [dev(a, k, kc) for a in range(3) for k in NEAR for kc in range(2)] + [dev(0, 0, 1)]
    for peer in peers:
        pl.semaphore_signal(barrier, 1, device_id=peer, device_id_type=MESH)

    loads = [
        pltpu.make_async_copy(src, dst, wsem.at[i])
        for i, (src, dst) in enumerate(
            (
                (k_hbm, k_ref), (v_hbm, v_ref), (kg_hbm, kg_ref), (rtab_hbm, rtab_ref), (ctab_hbm, ctab_ref),
                (ids_hbm, ids_ref), (q_hbm, q_ref), (qg_hbm, qg_ref), (gate_hbm, gate_ref), (res_hbm, res_ref),
                (mix_hbm, mix_ref), (ffn_hbm, ffn_ref), (post_hbm, post_ref),
                (wo_hbm, wo), (wg_hbm.at[0], wg), (wu_hbm.at[0], wu), (wd_hbm.at[0], wd),
            )
        )
    ]
    for load in loads:
        load.start()

    def loaded(first_load, last_load):
        for load in loads[first_load:last_load]:
            load.wait()

    lane = lax.broadcasted_iota(jnp.int32, (TOK, 128), 1)
    even = (lane % 2) == 0
    low = lane < 64
    seg = jnp.where(
        (lax.broadcasted_iota(jnp.int32, (128, 128), 0) // 64)
        == (lax.broadcasted_iota(jnp.int32, (128, 128), 1) // 64),
        1.0 / 64.0,
        0.0,
    ).astype(BF16)
    loaded(0, 6)
    rt = rtab_ref[s]
    cos = jnp.concatenate([ctab_ref[0] + rt[0:1], ctab_ref[0] + rt[1:2]], axis=0)
    sin = jnp.concatenate([ctab_ref[1] + rt[2:3], ctab_ref[1] + rt[3:4]], axis=0)

    def turn(x, gain):
        x = x.astype(F32)
        sq = x * x
        hi = sq.astype(BF16)
        lo = (sq - hi.astype(F32)).astype(BF16)
        ms = jnp.dot(hi, seg, preferred_element_type=F32) + jnp.dot(
            lo, seg, preferred_element_type=F32
        )
        y = x * lax.rsqrt(ms + EPS) * gain
        swapped = jnp.where(even, pltpu.roll(y, 127, 1), pltpu.roll(y, 1, 1))
        return y * cos + swapped * sin

    kgain = jnp.concatenate([kg_ref[...], kg_ref[...]], axis=1)
    for p in range(2):
        cols = slice(p * 128, (p + 1) * 128)
        kv[p, 0, :, 0:128] = turn(k_ref[0, :, cols], kgain).astype(BF16)
        kv[p, 0, :, 128:256] = v_ref[0, :, cols]
        kv[p, :, :, 256:384] = jnp.ones((16, TOK, 128), BF16)

    pl.semaphore_wait(barrier, len(peers))

    def hop(p, axis, k, src, dst):
        return pltpu.make_async_remote_copy(
            src_ref=kv.at[p, src, :, pl.ds(0, 256)],
            dst_ref=kv.at[p, dst, :, pl.ds(0, 256)],
            send_sem=gs.at[p, dst // 4],
            recv_sem=gr.at[p, min(dst, 12)],
            device_id=dev(axis, k),
            device_id_type=MESH,
        )

    def gather_first(p, k1):
        return hop(p, PAIRS[p][0], k1, 0, k1)

    def gather_second(p, k2, k1):
        if k2 == 2:
            k = 1 if k1 < 2 else 3
            return hop(p, PAIRS[p][1], k, PLACE[k, k1], PLACE[2, k1])
        return hop(p, PAIRS[p][1], k2, k1, PLACE[k2, k1])

    for k1 in NEAR:
        for p in range(2):
            gather_first(p, k1).start()
    for k2 in (1, 3):
        for p in range(2):
            gather_second(p, k2, 0).start()

    for axis in range(3):
        for k in NEAR:
            pltpu.make_async_remote_copy(
                src_ref=ids_ref,
                dst_ref=ids_in.at[axis, k],
                send_sem=idsem.at[0],
                recv_sem=idsem.at[1],
                device_id=dev(axis, k),
                device_id_type=MESH,
            ).start()

    loaded(6, 13)
    qgain = jnp.concatenate([qg_ref[...], qg_ref[...]], axis=1)
    for b in range(8):
        t = turn(q_ref[0, :, b * 128 : (b + 1) * 128], qgain).astype(BF16).astype(F32) * 0.125
        flip = pltpu.roll(t, 64, 1)
        p, pos, i = b // 4, (b // 2) % 2, (b % 4) * 2
        if pos == 0:
            a0, a1 = jnp.where(low, t, 0.0), jnp.where(low, flip, 0.0)
        else:
            a0, a1 = jnp.where(low, 0.0, flip), jnp.where(low, 0.0, t)
        qp[p, i * 128 : (i + 1) * 128] = a0.astype(BF16)
        qp[p, (i + 1) * 128 : (i + 2) * 128] = a1.astype(BF16)

    for k1 in (1, 3, 2):
        for p in range(2):
            gather_first(p, k1).wait_recv()
            for k2 in (1, 3):
                gather_second(p, k2, k1).start()
    for p in range(2):
        gather_second(p, 1, 0).wait_recv()
        gather_second(p, 2, 0).start()

    tok_r = lax.broadcasted_iota(jnp.int32, (128, 128), 0)
    tok_c = lax.broadcasted_iota(jnp.int32, (128, 128), 1)
    before = (tok_r < tok_c).astype(F32).astype(BF16)
    slot_row = lax.broadcasted_iota(jnp.int32, (128, 128), 0)
    slot_col = lax.broadcasted_iota(jnp.int32, (128, SLOTS), 1).astype(F32)

    def route(pair):
        idt = [pair[k : k + 1, :] for k in range(2)]
        hot = [(t == tok_r).astype(F32) for t in idt]
        cnt = [jnp.dot(h.astype(BF16), before, preferred_element_type=F32) for h in hot]
        cnt[1] = cnt[1] + jnp.sum(hot[0], axis=1, keepdims=True)
        rank = [jnp.sum(h * c, axis=0, keepdims=True).astype(jnp.int32) for h, c in zip(hot, cnt)]
        return list(zip(idt, rank))

    def places(e, rank, axes):
        at = (e // 32, (e // 8) % 4, (e // 2) % 4)
        rel = [(at[a] - mine[a] + 4) % 4 for a in axes]
        return rel[0], (e % 2 + core) % 2, (rel[1] * 4 + rel[2]) * 4 + rank

    def pick(p, k, routed):
        slots = []
        for e, rank in routed:
            plane, kc, r = places(e, rank, PARTS[p][0])
            slots.append(jnp.where(plane == 0, kc * 64 + r, -1))
        disp[p, k] = ((slot_row == slots[0]) | (slot_row == slots[1])).astype(F32).astype(BF16)

    own = route(ids_ref[...])
    for p, (axes, _, _) in enumerate(PARTS):
        pick(p, 0, own)
        for k, (e, rank) in enumerate(own):
            plane, kc, r = places(e, rank, axes)
            full = (kc * 4 + plane) * 64 + r
            col = jnp.transpose(jnp.broadcast_to(full.astype(F32), (128, 128)))[:, 0:1]
            comb[p, k] = (slot_col == col).astype(F32).astype(BF16)

    def stripe(first_place, count, fresh):
        for p in range(2):
            span = slice(first_place * 4, (first_place + count) * 4)
            n = count * 512
            keys = kv[p, span, :, 0:128].reshape(n, 128)
            vals = kv[p, span, :, 128:384].reshape(n, 256)
            for i in range(1024 // ROWS):
                r = slice(i * ROWS, (i + 1) * ROWS)
                sc = lax.dot_general(
                    qp[p, r, :], keys, (((1,), (1,)), ((), ())), preferred_element_type=F32
                )
                top = jnp.broadcast_to(jnp.max(sc, axis=1, keepdims=True), (ROWS, 128))
                if not fresh:
                    old = mx[p, r, :]
                    top = jnp.maximum(top, old)
                    fade = jnp.exp(old - top)
                mx[p, r, :] = top
                e = jnp.exp(sc - jnp.concatenate([top] * (n // 128), axis=1)).astype(BF16)
                o = jnp.dot(e, vals, preferred_element_type=F32)
                if not fresh:
                    o = o + acc[p, r, :] * jnp.concatenate([fade, fade], axis=1)
                acc[p, r, :] = o

    stripe(0, 1, True)

    def relay(k2, k1):
        for p in range(2):
            gather_second(p, k2, k1).wait_recv()
            gather_second(p, 2, k1).start()

    def arrive(*pieces):
        for k2, k1 in pieces:
            for p in range(2):
                gather_second(p, k2, k1).wait_recv()

    relay(1, 1)
    drain(ids_in.at[:, pl.ds(1, 3)], idsem.at[1])
    for p in range(3):
        for k in NEAR:
            pick(p, k, route(ids_in[p, k]))
    relay(3, 3)
    arrive((3, 0), (3, 1))
    stripe(1, 1, False)
    relay(3, 2)
    arrive((1, 3), (1, 2))
    stripe(2, 1, False)
    for p in range(2):
        drain(kv.at[p, pl.ds(12, 4), :, pl.ds(0, 256)], gr.at[p, 12])
    stripe(3, 1, False)

    for b in range(8):
        p, pos, i = b // 4, (b // 2) % 2, (b % 4) * 2
        o = []
        for j in (i, i + 1):
            r = slice(j * 128, (j + 1) * 128)
            o.append(acc[p, r, 0:128] / acc[p, r, 128:256])
        if pos == 0:
            a = jnp.where(low, o[0], pltpu.roll(o[1], 64, 1))
        else:
            a = jnp.where(low, pltpu.roll(o[0], 64, 1), o[1])
        att[:, b * 128 : (b + 1) * 128] = a.astype(BF16)

    loaded(13, 14)
    projected = jnp.dot(att[...], wo[...], preferred_element_type=F32)
    fr = (res_ref[0].astype(F32) + rms(projected) * mix_ref[...]).astype(BF16)
    first[...] = fr
    normed[...] = (rms(fr.astype(F32)) * ffn_ref[...]).astype(BF16)

    def cols_of(p):
        return pl.ds(PARTS[p][1], PARTS[p][2])

    def remote(src, dst, ss, rs, device):
        return pltpu.make_async_remote_copy(
            src_ref=src, dst_ref=dst, send_sem=ss, recv_sem=rs, device_id=device, device_id_type=MESH
        )

    def stage1(p, k1, relayed):
        axis = PARTS[p][0][0]
        c = cols_of(p)
        if relayed:
            r = pl.ds(0 if k1 == 1 else 64, 64)
            return remote(line.at[k1, r, c], line.at[2, r, c], f1s.at[p], f1r.at[p, 1], dev(axis, k1))
        return remote(normed.at[:, c], line.at[k1, :, c], f1s.at[p], f1r.at[p, k1 - 1], dev(axis, k1))

    def last1(u, k1):
        w, p = u
        n = w * 3 + p
        c = cols_of(p)
        src, dst = inboxr.at[w, k1, :, c], outr.at[w, k1, :, c]
        if k1 == 0:
            return pltpu.make_async_copy(src, dst, r3r.at[n])
        return remote(src, dst, sent.at[n, 1], r3r.at[n], dev(PARTS[p][0][0], 4 - k1))

    def stage2(u, k2, k1, back):
        w, p = u
        n = w * 3 + p
        axis = PARTS[p][0][1]
        c = cols_of(p)
        r = pl.ds(k2 * 16, 16)
        if back:
            return remote(midr.at[w, k2, k1, :, c], inboxr.at[w, k1, r, c], sent.at[n, 1], r2r.at[n, k1], dev(axis, 4 - k2))
        g = k1 if p == 2 else k2
        return remote(inbox.at[w, k1, r, c], mid.at[w, k2, k1, :, c], sent.at[n, 0], f2r.at[n, g], dev(axis, k2))

    def stage3(u, g, zero, k3, back):
        w, p = u
        n = w * 3 + p
        axis = PARTS[p][0][2]
        c = cols_of(p)
        r = pl.ds(k3 * 4, 4)
        box, deep, far = (inboxr, midr, ys) if back else (inbox, mid, xs)
        if p == 2:
            q = pl.ds(g * 4, 4)
            if zero:
                here, there = box.at[w, g, r, c], far.at[w, k3, 0, q, c]
            else:
                here, there = deep.at[w, pl.ds(1, 3), g, r, c], far.at[w, k3, pl.ds(1, 3), q, c]
        else:
            here = box.at[w, :, r, c] if zero else deep.at[w, g, :, r, c]
            there = far.at[w, g, :, r, c] if p == 0 else far.at[w, :, k3, pl.ds(g * 4, 4), c]
        if back:
            sem = r1z.at[n] if zero else r1r.at[n, g]
            if k3 == 0 and w == 0:
                return pltpu.make_async_copy(there, here, sem)
            return remote(there, here, sent.at[n, 1], sem, dev(axis, 4 - k3, w))
        if (k3, w) == (0, 0):
            return pltpu.make_async_copy(here, there, f3r.at[n])
        return remote(here, there, sent.at[n, 0], f3r.at[n], dev(axis, k3, w))

    def fan(u, g, zero, back):
        if not back:
            return [(k3, stage3(u, g, zero, k3, back)) for k3 in (1, 3, 0, 2)]

        @pl.when(u[0] == 0)
        def _():
            stage3((0, u[1]), g, zero, 0, back).start()

        @pl.when(u[0] == 1)
        def _():
            stage3((1, u[1]), g, zero, 0, back).start()

        return [(k3, stage3(u, g, zero, k3, back)) for k3 in (1, 3, 2)]

    def go(items):
        for far in (False, True):
            for k, copy in items:
                if (k == 2) == far:
                    copy.start()

    for k1 in (1, 3):
        for p in range(3):
            stage1(p, k1, False).start()

    def pack(p, k1):
        c = slice(PARTS[p][1], PARTS[p][1] + PARTS[p][2])
        rows = normed[:, c] if k1 == 0 else line[k1, :, c]
        packed = jnp.dot(disp[p, k1], rows, preferred_element_type=F32).astype(BF16)
        inbox[:, k1, :, c] = packed.reshape(2, 64, PARTS[p][2])
        return [(k2, stage2((w, p), k2, k1, False)) for w in range(2) for k2 in (1, 3, 2)]

    def packs(k1):
        items = []
        for p in range(3):
            items += pack(p, k1)
        go(items)

    packs(0)
    for k1 in (1, 3):
        for p in range(3):
            drain(line.at[k1, :, cols_of(p)], f1r.at[p, k1 - 1])
            stage1(p, k1, True).start()
    packs(1)
    packs(3)
    for p in range(3):
        drain(line.at[2, :, cols_of(p)], f1r.at[p, 1])
    packs(2)
    for w in range(2):
        items = []
        for p in range(3):
            for g in range(4) if p == 2 else range(1):
                items += fan((w, p), g, True, False)
        go(items)
    for w in range(2):
        for i in range(4):
            items = []
            for p in range(3):
                u = (w, p)
                n = w * 3 + p
                c = cols_of(p)
                g = (0, 1, 3, 2)[i]
                if p == 2:
                    drain(mid.at[w, pl.ds(1, 3), g, :, c], f2r.at[n, g])
                elif i > 0:
                    drain(mid.at[w, g, :, :, c], f2r.at[n, g])
                if p == 2 or i > 0:
                    items += fan(u, g, False, False)
            go(items)

    def middle(waves):
        for w in waves:
            for i in range(4):
                items = []
                for p in range(3):
                    u = (w, p)
                    n = w * 3 + p
                    c = cols_of(p)
                    g = (NEAR + (0,))[i]
                    if p == 2:
                        drain(midr.at[w, pl.ds(1, 3), g, :, c], r1r.at[n, g])
                        items += [(k2, stage2(u, k2, g, True)) for k2 in (1, 3, 2)]
                    elif g > 0:
                        drain(midr.at[w, g, :, :, c], r1r.at[n, g])
                        items += [(g, stage2(u, g, k1, True)) for k1 in NEAR + (0,)]
                go(items)

    def final(w):
        for p in range(3):
            drain(inboxr.at[w, :, pl.ds(0, 16), cols_of(p)], r1z.at[w * 3 + p])
        for k1 in NEAR + (0,):
            for p in range(3):
                drain(inboxr.at[w, k1, pl.ds(16, 48), cols_of(p)], r2r.at[w * 3 + p, k1])
                last1((w, p), k1).start()

    def finish(*steps):
        for step, w in steps:
            if step == 2:
                middle((w,))
            else:
                final(w)

    for turn_no in range(2):
        w = (1 - core + turn_no) % 2
        if turn_no == 0:
            loaded(14, 17)
        for p in range(3):
            drain(xs.at[w, :, :, :, cols_of(p)], f3r.at[w * 3 + p])
        x = xs[w].reshape(256, D)
        gate = jnp.dot(x, wg[...], preferred_element_type=F32)
        up = jnp.dot(x, wu[...], preferred_element_type=F32)
        hidden = (jax.nn.silu(gate) * up).astype(BF16)
        for p in range(3):
            u = (w, p)
            c = slice(PARTS[p][1], PARTS[p][1] + PARTS[p][2])
            ys[w, :, :, :, c] = (
                jnp.dot(hidden, wd[:, c], preferred_element_type=F32)
                .astype(BF16)
                .reshape(4, 4, 16, PARTS[p][2])
            )
            items = []
            for g in NEAR + (0,):
                if p == 2 or g > 0:
                    items += fan(u, g, False, True)
            for g in range(4) if p == 2 else range(1):
                items += fan(u, g, True, True)
            go(items)
        if turn_no == 0:
            pl.when(core == 1)(lambda: middle((0,)))
        else:
            pl.when(core == 1)(lambda: finish((2, 1), (3, 0), (3, 1)))
            pl.when(core == 0)(lambda: finish((2, 0), (3, 0), (2, 1), (3, 1)))


    g0, g1 = [jnp.transpose(jnp.broadcast_to(gate_ref[k : k + 1, :], (128, 128))) for k in range(2)]
    sums = [None] * 3
    for w in range(2):
        for p in range(3):
            c = slice(PARTS[p][1], PARTS[p][1] + PARTS[p][2])
            half = slice(w * 256, (w + 1) * 256)
            wide = PARTS[p][2] // 128
            drain(outr.at[w, :, :, cols_of(p)], r3r.at[w * 3 + p])
            back = outr[w, :, :, c].reshape(256, PARTS[p][2])
            a0 = jnp.dot(comb[p, 0, :, half], back, preferred_element_type=F32)
            a1 = jnp.dot(comb[p, 1, :, half], back, preferred_element_type=F32)
            term = jnp.concatenate([g0] * wide, axis=1) * a0 + jnp.concatenate([g1] * wide, axis=1) * a1
            if w == 0:
                tot[:, c] = term
            else:
                sums[p] = tot[:, c] + term
    total = jnp.concatenate(sums, axis=1)
    out_ref[0] = (first[...].astype(F32) + rms(total) * post_ref[...]).astype(BF16)

    for p in range(2):
        drain(kv.at[p, pl.ds(0, 3), :, pl.ds(0, 256)], gs.at[p, 0])
        for i in range(1, 4):
            drain(kv.at[p, pl.ds(0, 4), :, pl.ds(0, 256)], gs.at[p, i])
    drain(ids_in.at[:, pl.ds(1, 3)], idsem.at[0])
    for p in range(3):
        drain(wo.at[pl.ds(0, 384), cols_of(p)], f1s.at[p])
    for w, p in UNITS:
        n = w * 3 + p
        c = cols_of(p)
        drain(wo.at[pl.ds(0, 384 + w * 64), c], sent.at[n, 0])
        drain(wo.at[pl.ds(0, 576 + w * 64), c], sent.at[n, 1])


def shards(
    queries, keys, values, q_gain, k_gain, residual, out_weight, mix_gain, ffn_gain, post_gain,
    expert_ids, expert_gate, w_gate, w_up, w_down,
):
    rows, cols = tables()
    vm = pl.BlockSpec(memory_space=pltpu.VMEM)
    hbm = pl.BlockSpec(memory_space=pltpu.HBM)
    sem = pltpu.SemaphoreType.DMA
    box = pltpu.VMEM((2, 4, 64, D), BF16)
    deep = pltpu.VMEM((2, 4, 4, 16, D), BF16)
    return pl.pallas_call(
        kernel,
        out_shape=jax.ShapeDtypeStruct((1, TOK, D), BF16),
        in_specs=[hbm] * 17,
        out_specs=vm,
        scratch_shapes=[
            pltpu.VMEM((1, TOK, 256), BF16), pltpu.VMEM((1, TOK, 256), BF16), pltpu.VMEM((1, 64), F32),
            pltpu.VMEM((16, 8, 128), F32), pltpu.VMEM((2, 64, 128), F32),
            pltpu.VMEM((1, TOK, 1024), BF16), pltpu.VMEM((1, 64), F32),
            pltpu.VMEM((2, TOK), jnp.int32), pltpu.VMEM((2, TOK), F32), pltpu.VMEM((1, TOK, D), BF16),
            pltpu.VMEM((1, D), F32), pltpu.VMEM((1, D), F32), pltpu.VMEM((1, D), F32),
            pltpu.VMEM((1024, D), BF16),
            pltpu.VMEM((D, 512), BF16),
            pltpu.VMEM((D, 512), BF16),
            pltpu.VMEM((512, D), BF16),
            pltpu.VMEM((2, 1024, 128), BF16),
            pltpu.VMEM((2, 16, TOK, 384), BF16),
            pltpu.VMEM((2, 1024, 128), F32),
            pltpu.VMEM((2, 1024, 256), F32),
            pltpu.VMEM((TOK, 1024), BF16),
            pltpu.VMEM((TOK, D), BF16),
            pltpu.VMEM((TOK, D), BF16),
            pltpu.VMEM((3, 4, 128, 128), BF16),
            pltpu.VMEM((3, 2, 128, SLOTS), BF16),
            pltpu.VMEM((3, 4, 2, TOK), jnp.int32),
            pltpu.VMEM((4, TOK, D), BF16),
            box, deep, deep, deep, deep, box, box,
            pltpu.VMEM((TOK, D), F32),
            sem((17,)), sem((2,)),
            sem((2, 4)), sem((2, 13)),
            sem((3,)), sem((3, 3)), sem((6, 4)), sem((6,)),
            sem((6, 4)), sem((6,)), sem((6, 4)), sem((6,)),
            sem((6, 2)),
        ],
        compiler_params=pltpu.CompilerParams(
            collective_id=0, has_side_effects=True, vmem_limit_bytes=LIMIT
        ),
        name="layer",
    )(
        keys, values, k_gain[None], jnp.asarray(rows), jnp.asarray(cols), queries, q_gain[None],
        expert_ids[0].T, expert_gate[0].T, residual, mix_gain[None], ffn_gain[None], post_gain[None],
        out_weight, w_gate, w_up, w_down,
    )


def solution(mesh):
    return jax.shard_map(
        shards,
        mesh=mesh,
        in_specs=(
            P("dp", "sp", None), P("dp", "sp", None), P("dp", "sp", None), P(), P(),
            P("dp", "sp", None), P(), P(), P(), P(),
            P("dp", "sp", None), P("dp", "sp", None),
            P(("sp", "dp"), None, None), P(("sp", "dp"), None, None), P(("sp", "dp"), None, None),
        ),
        out_specs=P("dp", "sp", None),
        check_vma=False,
    )
```
